256 devices in a mesh: ra: 2 (over core), cb: 32 (over z, x), dp: 4 (over y).
Axes of the slice: x: 4, y: 4, z: 8, core: 2. Of those that a mesh axis runs over, the one named last changes fastest.
Arguments:
- residual_in: bfloat16 [1024, 4096], P('dp', 'cb'), may hold values from -220 to 220, as said below
- gain_in: float32 [4096], P('cb'), may hold values from 0.1 to 1.9
- shift_in: float32 [4096], P('cb'), may hold values from -3 to 3
- up_weight: bfloat16 [4096, 16384], P('cb', 'ra'), may hold values from -0.09375 to 0.09375
- down_weight: bfloat16 [16384, 4096], P('ra', 'cb'), may hold values from -0.046875 to 0.046875
- gain_out: float32 [4096], P('cb'), may hold values from 0.1 to 1.9
- shift_out: float32 [4096], P('cb'), may hold values from -3 to 3
Outputs:
- layer_out: bfloat16 [1024, 4096], P('dp', 'cb')
The draws below stay inside these ranges and needn't reach their ends.
Inputs may be any that keep to these rules, and one draw needn't show every extreme that they name: `residual_in`: real-valued activations.
All inputs are finite; a program needn't handle non-finite values.
Results may differ from the reference program's by a relative error of at most 0.0065.
Values may be sent and summed in bfloat16 or wider, within the bound.
A program may use at most 64 MiB of HBM per device.

```python
import jax
import jax.numpy as jnp
from jax import lax

D = 4096
FF = 16384
TOKENS = 1024


def draw_residual_in(key, part):
    first, second, third = jax.random.split(key, 3)
    column = jnp.arange(D, dtype=jnp.float32) / D
    colscale = 0.5 * jnp.exp(jnp.log(6.0) * column) * jnp.exp(jax.random.uniform(second, (D,), jnp.float32, -0.35, 0.35))
    rowscale = jnp.exp(jax.random.uniform(third, (TOKENS, 1), jnp.float32, 0.0, jnp.log(10.0)))
    noise = jnp.clip(jax.random.normal(first, (TOKENS, D), jnp.float32), -5.0, 5.0)
    values = rowscale * noise * colscale
    return values.astype(jnp.bfloat16)


def steps_of(stream_key, dims, shards, low, high):
    level = 1.0
    for axis_at, parts in shards:
        heights = jax.random.uniform(jax.random.fold_in(jax.random.fold_in(stream_key, 6), axis_at), (parts,), jnp.float32, low / len(shards), high / len(shards))
        level = level * jnp.repeat(jnp.exp(heights), dims[axis_at] // parts).reshape((-1,) + (1,) * (len(dims) - 1 - axis_at))
    return level


def bell_draw(rng, extent, scale, limit, shards=(), kind=jnp.bfloat16):
    level = steps_of(rng, extent, shards, -0.22, 0.18) if shards else 1.0
    values = jax.random.normal(rng, extent, jnp.float32) * scale * level
    return jnp.minimum(jnp.maximum(values, -limit), limit).astype(kind)


def setup_inputs(seed: int = 0) -> dict:
    arg_keys = jax.random.split(jax.random.key(seed), 8)
    residual_in = draw_residual_in(jax.random.fold_in(arg_keys[7], 71), 0)
    gain_in = jnp.clip(1.0 + 0.18 * jax.random.normal(arg_keys[1], (D,), jnp.float32), 0.1, 1.9)
    shift_in = bell_draw(arg_keys[2], (D,), 0.5, 3.0, ((0, 32),), jnp.float32)
    up_weight = bell_draw(arg_keys[3], (D, FF), D ** -0.5, 0.09375, ((0, 32), (1, 2)))
    down_weight = bell_draw(arg_keys[4], (FF, D), FF ** -0.5, 0.046875, ((0, 2), (1, 32)))
    gain_out = jnp.clip(1.0 + 0.18 * jax.random.normal(arg_keys[5], (D,), jnp.float32), 0.1, 1.9)
    shift_out = bell_draw(arg_keys[6], (D,), 0.5, 3.0, ((0, 32),), jnp.float32)
    return {"residual_in": residual_in, "gain_in": gain_in, "shift_in": shift_in, "up_weight": up_weight, "down_weight": down_weight, "gain_out": gain_out, "shift_out": shift_out}


def layer_norm(values, gain, shift):
    mean = lax.optimization_barrier(jnp.mean(values, axis=-1, keepdims=True))
    centred = values - mean
    spread = lax.optimization_barrier(jnp.mean(centred * centred, axis=-1, keepdims=True))
    return centred * jax.lax.rsqrt(spread + 1e-05) * gain + shift

def reference(residual_in, gain_in, shift_in, up_weight, down_weight, gain_out, shift_out):
    normed = layer_norm(residual_in.astype(jnp.float32), gain_in, shift_in).astype(jnp.bfloat16)
    pre = jnp.dot(normed, up_weight, preferred_element_type=jnp.float32)
    hidden = jnp.square(jax.nn.relu(pre)).astype(jnp.bfloat16)
    branch = jnp.dot(hidden, down_weight, preferred_element_type=jnp.float32)
    total = 2.0 ** 0.25 * normed.astype(jnp.float32) + branch
    return layer_norm(total, gain_out, shift_out).astype(jnp.bfloat16)
```

```python
import functools

import jax
import jax.numpy as jnp
from jax import lax
from jax.experimental import pallas as pl
from jax.experimental.pallas import tpu as pltpu
from jax.sharding import Mesh
from jax.sharding import PartitionSpec as P

CB = ("cb_0", "cb_1")
MESH = pl.DeviceIdType.MESH
NC = 4
ORDER = (0, 2, 1, 3)
EPS = 1e-05
F32 = jnp.float32
BF16 = jnp.bfloat16


def hops(c, di, nz):
    return nz // 2 if (c < NC // 2) == (di == 0) else nz // 2 - 1


def columns_to_rows(a, b):
    n = a.shape[0]
    lane = lax.broadcasted_iota(jnp.int32, (n, 128), 1)
    both = jnp.where(lane == 0, a, jnp.where(lane == 1, b, 0.0))
    return both.T[0:2, :]


def row_to_lanes(row):
    return jnp.broadcast_to(row, (128, row.shape[1])).T


def combine(stats, count):
    sums, squares = stats[:, 0, :], stats[:, 1, :]
    parts = stats.shape[0]
    mean = jnp.sum(sums, axis=0, keepdims=True) / (parts * count)
    apart = sums / count - mean
    total = jnp.sum(squares, axis=0, keepdims=True) + count * jnp.sum(apart * apart, axis=0, keepdims=True)
    return mean, lax.rsqrt(total / (parts * count) + EPS)


def kernel(
    nz, nx, res_hbm, gi_hbm, si_hbm, up_hbm, dn_hbm, go_hbm, so_hbm, out_hbm,
    raw, gi, si, go, so, wup, wdn, st1, normed, rsb, rrb, hid, bacc, xsend, xrecv, sb, rb, st2, outv,
    local_sem, raw_sem, g_sem, up_sem, dn_sem, st1_sem, n_sem, rs_sem, ag_sem, x_sem, br_sem, st2_sem, out_sem,
):
    half = res_hbm.shape[0] // 2
    width = res_hbm.shape[1]
    nq = nz // 2
    h = half // nq
    depth = nx * width
    fc = wdn.shape[0]
    cw = fc // NC
    lm = nz // 2

    r = lax.axis_index("ra")
    z = lax.axis_index("cb_0")
    x = lax.axis_index("cb_1")
    y = lax.axis_index("dp")
    p = lax.rem(y, 2)
    other = 1 - r
    xs = [lax.rem(x + k, nx) for k in range(nx)]
    zs = [lax.rem(z + k, nz) for k in range(nz)]
    ys = [y, y + 1 - 2 * p]
    ps = [p, 1 - p]
    sibling = (other, z, x, y)

    barrier = pltpu.get_barrier_semaphore()
    greeted = [sibling]
    greeted += [(r, z, xs[dx], ys[dj]) for dj in range(2) for dx in range(nx) if dx or dj]
    greeted += [(r, zs[dz], x, y) for dz in range(1, nz)]
    for peer in greeted:
        pl.semaphore_signal(barrier, inc=1, device_id=peer, device_id_type=MESH)

    mine = pl.ds(pl.multiple_of(r * half, half), half)
    own = pl.ds(pl.multiple_of(x * width, width), width)
    first = [
        pltpu.make_async_copy(res_hbm.at[mine, :], raw.at[x, p], local_sem.at[0]),
        pltpu.make_async_copy(gi_hbm, gi.at[x], local_sem.at[1]),
        pltpu.make_async_copy(si_hbm, si.at[x], local_sem.at[2]),
        pltpu.make_async_copy(go_hbm, go, local_sem.at[3]),
        pltpu.make_async_copy(so_hbm, so, local_sem.at[4]),
    ]
    for copy in first:
        copy.start()

    def share(xd):
        return (xd * 2 + p) * fc

    up_own = []
    for c in range(NC):
        cols = pl.ds(pl.multiple_of(share(x) + c * cw, cw), cw)
        up_own.append(pltpu.make_async_copy(up_hbm.at[:, cols], wup.at[c, own, :], local_sem.at[5 + c]))
        up_own[-1].start()
    dn_own = pltpu.make_async_copy(
        dn_hbm.at[pl.ds(pl.multiple_of(share(x), fc), fc), :], wdn.at[:, own], local_sem.at[5 + NC]
    )
    dn_own.start()

    sent = []

    def remote(src, dst, sems, index, peer):
        copy = pltpu.make_async_remote_copy(
            src_ref=src, dst_ref=dst, send_sem=sems.at[(0, *index)], recv_sem=sems.at[(1, *index)],
            device_id=peer, device_id_type=MESH,
        )
        copy.start()
        sent.append(copy)

    def arrived(dst, sems, index):
        pltpu.make_async_remote_copy(
            src_ref=dst, dst_ref=dst, send_sem=sems.at[(0, *index)], recv_sem=sems.at[(1, *index)],
            device_id=sibling, device_id_type=MESH,
        ).wait_recv()

    for copy in first:
        copy.wait()
    pl.semaphore_wait(barrier, len(greeted))

    for dj in range(2):
        for dx in range(nx):
            if dx or dj:
                remote(raw.at[x, p], raw.at[x, p], raw_sem, (dj, dx), (r, z, xs[dx], ys[dj]))
    for dx in range(1, nx):
        peer = (r, z, xs[dx], y)
        remote(gi.at[x], gi.at[x], g_sem, (0, dx), peer)
        remote(si.at[x], si.at[x], g_sem, (1, dx), peer)
    for c in ORDER:
        for dx in range(1, nx):
            cols = pl.ds(pl.multiple_of(share(xs[dx]) + c * cw, cw), cw)
            remote(up_hbm.at[:, cols], wup.at[c, own, :], up_sem, (c, dx), (r, z, xs[dx], y))
    for dx in range(1, nx):
        rows = pl.ds(pl.multiple_of(share(xs[dx]), fc), fc)
        remote(dn_hbm.at[rows, :], wdn.at[:, own], dn_sem, (dx,), (r, z, xs[dx], y))

    for dj in range(2):
        for dx in range(nx):
            if dx or dj:
                arrived(raw.at[xs[nx - dx] if dx else x, ps[dj]], raw_sem, (dj, dx))
    for j in range(2):
        values = [raw[k, j].astype(F32) for k in range(nx)]
        total = jnp.sum(functools.reduce(jnp.add, values), axis=1, keepdims=True)
        mean = total / depth
        apart = [v - mean for v in values]
        square = jnp.sum(functools.reduce(jnp.add, [a * a for a in apart]), axis=1, keepdims=True)
        st1[z, :, j * half : (j + 1) * half] = columns_to_rows(total, square)
    for dz in range(1, nz):
        remote(st1.at[z], st1.at[z], st1_sem, (dz,), (r, zs[dz], x, y))
    for dx in range(1, nx):
        arrived(gi.at[xs[nx - dx]], g_sem, (0, dx))
        arrived(si.at[xs[nx - dx]], g_sem, (1, dx))
    for dz in range(1, nz):
        arrived(st1.at[zs[nz - dz]], st1_sem, (dz,))
    mean, scale = combine(st1[...], depth)
    for j in range(2):
        part = slice(j * half, (j + 1) * half)
        mean_j, scale_j = row_to_lanes(mean[:, part]), row_to_lanes(scale[:, part])
        for k in range(nx):
            v = (raw[k, j].astype(F32) - mean_j) * scale_j * gi[k] + si[k]
            normed[j * nq : (j + 1) * nq, r, :, k * width : (k + 1) * width] = v.astype(BF16).reshape(nq, h, width)
    remote(normed.at[:, r], normed.at[:, r], n_sem, (), sibling)
    arrived(normed.at[:, other], n_sem, ())

    def partial(d, c):
        return jnp.dot(normed[d].reshape(2 * h, depth), wup[c], preferred_element_type=F32)

    ready = set()

    def step_peer(di):
        return (r, zs[1] if di == 0 else zs[nz - 1], x, y)

    for s in range(lm):
        for c in ORDER:
            if c not in ready:
                ready.add(c)
                up_own[c].wait()
                for dx in range(1, nx):
                    arrived(wup.at[c, pl.ds(pl.multiple_of(xs[nx - dx] * width, width), width), :], up_sem, (c, dx))
            for di in range(2):
                length = hops(c, di, nz)
                if s < length:
                    ahead = length - s
                    value = partial(zs[ahead] if di == 0 else zs[nz - ahead], c)
                    if s:
                        arrived(rrb.at[c, di, s - 1], rs_sem, (c, di, s - 1))
                        value = value + rrb[c, di, s - 1].astype(F32)
                    rsb[c, di, s] = value.astype(BF16)
                    remote(rsb.at[c, di, s], rrb.at[c, di, s], rs_sem, (c, di, s), step_peer(di))
    for c in ORDER:
        value = partial(z, c)
        for di in range(2):
            last = hops(c, di, nz) - 1
            arrived(rrb.at[c, di, last], rs_sem, (c, di, last))
            value = value + rrb[c, di, last].astype(F32)
        hid[c, z] = jnp.square(jnp.maximum(value, 0.0)).astype(BF16)
        for di in range(2):
            remote(hid.at[c, z], hid.at[c, z], ag_sem, (c, di, 0), step_peer(di))

    dn_own.wait()
    for dx in range(1, nx):
        arrived(wdn.at[:, pl.ds(pl.multiple_of(xs[nx - dx] * width, width), width)], dn_sem, (dx,))

    def down(k):
        o = zs[k]
        value = jnp.dot(hid[0, o], wdn[0:cw, :], preferred_element_type=F32)
        for c in range(1, NC):
            value += jnp.dot(hid[c, o], wdn[c * cw : (c + 1) * cw, :], preferred_element_type=F32)
        bacc[o] = value.reshape(2, h, depth)
        xsend[o] = bacc[o, other].astype(BF16)
        remote(xsend.at[o], xrecv.at[o], x_sem, (k,), sibling)

    down(0)
    for s in range(1, lm + 1):
        for c in ORDER:
            for di in range(2):
                length = hops(c, di, nz)
                if s <= length:
                    o = zs[nz - s] if di == 0 else zs[s]
                    arrived(hid.at[c, o], ag_sem, (c, di, s - 1))
                    if s < length:
                        remote(hid.at[c, o], hid.at[c, o], ag_sem, (c, di, s), step_peer(di))
        down(s)
        if s < lm:
            down(nz - s)
    for k in range(nz):
        o = zs[k]
        arrived(xrecv.at[o], x_sem, (k,))
        sb[o] = (bacc[o, r] + xrecv[o].astype(F32)).astype(BF16)

    for dj in range(2):
        for dx in range(nx):
            if dx or dj:
                blocks = pl.ds(pl.multiple_of(ps[dj] * nq, nq), nq)
                cols = pl.ds(pl.multiple_of(xs[dx] * width, width), width)
                remote(sb.at[blocks, :, cols], rb.at[dj, dx], br_sem, (dj, dx), (r, z, xs[dx], ys[dj]))
    blocks = pl.ds(pl.multiple_of(p * nq, nq), nq)
    total = 2.0**0.25 * normed[blocks, r, :, own].astype(F32) + sb[blocks, :, own].astype(F32)
    for dj in range(2):
        for dx in range(nx):
            if dx or dj:
                arrived(rb.at[dj, dx], br_sem, (dj, dx))
                total = total + rb[dj, dx].astype(F32)
    total = total.reshape(half, width)
    sums = jnp.sum(total, axis=1, keepdims=True)
    apart = total - sums / width
    st2[0] = columns_to_rows(sums, jnp.sum(apart * apart, axis=1, keepdims=True))
    for k in range(1, nz * nx):
        remote(st2.at[0], st2.at[k], st2_sem, (k,), (r, zs[k // nx], xs[k % nx], y))
    for k in range(1, nz * nx):
        arrived(st2.at[k], st2_sem, (k,))
    mean, scale = combine(st2[...], width)
    outv[...] = ((total - row_to_lanes(mean)) * row_to_lanes(scale) * go[...] + so[...]).astype(BF16)
    keep = pltpu.make_async_copy(outv, out_hbm.at[mine, :], local_sem.at[6 + NC])
    keep.start()
    remote(outv, out_hbm.at[mine, :], out_sem, (), sibling)
    keep.wait()
    arrived(out_hbm.at[pl.ds(pl.multiple_of(other * half, half), half), :], out_sem, ())
    for copy in sent:
        copy.wait_send()


def per_device(nz, nx, residual_in, gain_in, shift_in, up_weight, down_weight, gain_out, shift_out):
    tokens, width = residual_in.shape
    half, nq, depth = tokens // 2, nz // 2, nx * width
    h = half // nq
    fc = up_weight.shape[1] // (2 * nx)
    cw = fc // NC
    dma = pltpu.SemaphoreType.DMA
    row = (1, width)
    return pl.pallas_call(
        functools.partial(kernel, nz, nx),
        out_shape=jax.ShapeDtypeStruct((tokens, width), BF16),
        in_specs=[pl.BlockSpec(memory_space=pl.ANY)] * 7,
        out_specs=pl.BlockSpec(memory_space=pl.ANY),
        scratch_shapes=[
            pltpu.VMEM((nx, 2, half, width), BF16),
            pltpu.VMEM((nx, *row), F32),
            pltpu.VMEM((nx, *row), F32),
            pltpu.VMEM(row, F32),
            pltpu.VMEM(row, F32),
            pltpu.VMEM((NC, depth, cw), BF16),
            pltpu.VMEM((fc, depth), BF16),
            pltpu.VMEM((nz, 2, 2 * half), F32),
            pltpu.VMEM((nz, 2, h, depth), BF16),
            pltpu.VMEM((NC, 2, nq, 2 * h, cw), BF16),
            pltpu.VMEM((NC, 2, nq, 2 * h, cw), BF16),
            pltpu.VMEM((NC, nz, 2 * h, cw), BF16),
            pltpu.VMEM((nz, 2, h, depth), F32),
            pltpu.VMEM((nz, h, depth), BF16),
            pltpu.VMEM((nz, h, depth), BF16),
            pltpu.VMEM((nz, h, depth), BF16),
            pltpu.VMEM((2, nx, nq, h, width), BF16),
            pltpu.VMEM((nz * nx, 2, half), F32),
            pltpu.VMEM((half, width), BF16),
            dma((7 + NC,)),
            dma((2, 2, nx)),
            dma((2, 2, nx)),
            dma((2, NC, nx)),
            dma((2, nx)),
            dma((2, nz)),
            dma((2,)),
            dma((2, NC, 2, nq)),
            dma((2, NC, 2, nq)),
            dma((2, nz)),
            dma((2, 2, nx)),
            dma((2, nz * nx)),
            dma((2,)),
        ],
        compiler_params=pltpu.CompilerParams(collective_id=0, has_side_effects=True),
    )(
        residual_in, gain_in.reshape(row), shift_in.reshape(row), up_weight, down_weight,
        gain_out.reshape(row), shift_out.reshape(row),
    )


def solution(mesh):
    nz, nx = 8, 4
    split = Mesh(
        mesh.devices.reshape(mesh.shape["ra"], nz, nx, mesh.shape["dp"]), ("ra", "cb_0", "cb_1", "dp")
    )
    placed = (P("dp", CB), P(CB), P(CB), P(CB, "ra"), P("ra", CB), P(CB), P(CB))
    return jax.shard_map(
        functools.partial(per_device, nz, nx), mesh=split, in_specs=placed, out_specs=P("dp", CB), check_vma=False
    )
```

```python
import functools

import jax
import jax.numpy as jnp
from jax import lax
from jax.experimental import pallas as pl
from jax.experimental.pallas import tpu as pltpu
from jax.sharding import Mesh
from jax.sharding import PartitionSpec as P

CB = ("cb_0", "cb_1")
MESH = pl.DeviceIdType.MESH
NC = 4
ORDER = (0, 2, 1, 3)
EPS = 1e-05
F32 = jnp.float32
BF16 = jnp.bfloat16


def hops(c, di, nz):
    return nz // 2 if (c < NC // 2) == (di == 0) else nz // 2 - 1


def columns_to_rows(a, b):
    n = a.shape[0]
    lane = lax.broadcasted_iota(jnp.int32, (n, 128), 1)
    both = jnp.where(lane == 0, a, jnp.where(lane == 1, b, 0.0))
    return both.T[0:2, :]


def row_to_lanes(row):
    return jnp.broadcast_to(row, (128, row.shape[1])).T


def combine(stats, count):
    sums, squares = stats[:, 0, :], stats[:, 1, :]
    parts = stats.shape[0]
    mean = jnp.sum(sums, axis=0, keepdims=True) / (parts * count)
    apart = sums / count - mean
    total = jnp.sum(squares, axis=0, keepdims=True) + count * jnp.sum(apart * apart, axis=0, keepdims=True)
    return mean, lax.rsqrt(total / (parts * count) + EPS)


def kernel(
    nz, nx, res_hbm, gi_hbm, si_hbm, up_hbm, dn_hbm, go_hbm, so_hbm, out_ref,
    raw, gi, si, go, so, wup, wdn, st1, normed, pbuf, rsb, rrb, hid, bacc, xsend, xrecv, sb, rb, st2, tot,
    local_sem, raw_sem, rawf_sem, g_sem, up_sem, upf_sem, dn_sem, st1_sem, rs_sem, ag_sem, x_sem, br_sem, st2_sem, tot_sem,
):
    half = res_hbm.shape[0] // 2
    width = res_hbm.shape[1]
    nq = nz // 2
    h = half // nq
    depth = nx * width
    fc = wdn.shape[0]
    cw = fc // NC
    lm = nz // 2

    r = lax.axis_index("ra")
    z = lax.axis_index("cb_0")
    x = lax.axis_index("cb_1")
    y = lax.axis_index("dp")
    q = lax.rem(y, 2)
    pf = lax.rem(lax.div(y + 1, 2), 2)
    w = lax.div(y, 2)
    yw = 3 - y
    other = 1 - r
    xs = [lax.rem(x + k, nx) for k in range(nx)]
    zs = [lax.rem(z + k, nz) for k in range(nz)]
    ys = [y, y + 1 - 2 * q]
    qs = [q, 1 - q]
    sibling = (other, z, x, y)
    partner = (r, z, x, yw)

    def source(dx):
        return xs[nx - dx] if dx else x

    barrier = pltpu.get_barrier_semaphore()
    greeted = [sibling, partner]
    greeted += [(r, z, xs[dx], ys[dj]) for dj in range(2) for dx in range(nx) if dx or dj]
    greeted += [(c, zs[dz], x, y) for dz in range(1, nz) for c in (r, other)]
    for peer in greeted:
        pl.semaphore_signal(barrier, inc=1, device_id=peer, device_id_type=MESH)

    own = pl.ds(pl.multiple_of(x * width, width), width)
    first = [
        pltpu.make_async_copy(res_hbm.at[0:half, :], raw.at[0, x, q], local_sem.at[0]),
        pltpu.make_async_copy(res_hbm.at[half : 2 * half, :], raw.at[1, x, q], local_sem.at[1]),
        pltpu.make_async_copy(gi_hbm, gi.at[x], local_sem.at[2]),
        pltpu.make_async_copy(si_hbm, si.at[x], local_sem.at[3]),
        pltpu.make_async_copy(go_hbm, go, local_sem.at[4]),
        pltpu.make_async_copy(so_hbm, so, local_sem.at[5]),
    ]
    for copy in first:
        copy.start()

    def share(xd):
        return (xd * 2 + pf) * fc

    up_own = []
    for c in range(NC):
        cols = pl.ds(pl.multiple_of(share(x) + c * cw, cw), cw)
        up_own.append(pltpu.make_async_copy(up_hbm.at[:, cols], wup.at[c, own, :], local_sem.at[6 + c]))
        up_own[-1].start()
    dn_own = pltpu.make_async_copy(
        dn_hbm.at[pl.ds(pl.multiple_of(share(x), fc), fc), :], wdn.at[:, own], local_sem.at[6 + NC]
    )
    dn_own.start()

    sent = []

    def describe(src, dst, sems, index, peer):
        return pltpu.make_async_remote_copy(
            src_ref=src, dst_ref=dst, send_sem=sems.at[(0, *index)], recv_sem=sems.at[(1, *index)],
            device_id=peer, device_id_type=MESH,
        )

    def remote(src, dst, sems, index, peer):
        copy = describe(src, dst, sems, index, peer)
        copy.start()
        sent.append((copy, None))

    def remote_if(condition, src, dst, sems, index, peer):
        copy = describe(src, dst, sems, index, peer)
        pl.when(condition)(copy.start)
        sent.append((copy, condition))

    def arrived(dst, sems, index):
        describe(dst, dst, sems, index, sibling).wait_recv()

    for copy in first:
        copy.wait()
    pl.semaphore_wait(barrier, len(greeted))

    hw = width // 2

    def up_rows(xd, part):
        return pl.ds(pl.multiple_of(xd * width + part * hw, hw), hw)

    for dj in range(2):
        for dx in range(nx):
            if dx or dj:
                remote(raw.at[r, x, q], raw.at[r, x, q], raw_sem, (dj, dx), (r, z, xs[dx], ys[dj]))
    for dx in range(1, nx):
        peer = (r, z, xs[dx], y)
        remote(gi.at[x], gi.at[x], g_sem, (0, dx), peer)
        remote(si.at[x], si.at[x], g_sem, (1, dx), peer)
    for c in ORDER:
        for dx in range(1, nx):
            cols = pl.ds(pl.multiple_of(share(xs[dx]) + c * cw, cw), cw)
            rows = pl.ds(pl.multiple_of(w * hw, hw), hw)
            remote(up_hbm.at[rows, cols], wup.at[c, up_rows(x, w), :], up_sem, (c, dx), (r, z, xs[dx], y))

    def forward_up(c):
        for dx in range(1, nx):
            block = wup.at[c, up_rows(source(dx), w), :]
            arrived(block, up_sem, (c, dx))
            remote(block, block, upf_sem, (c, dx), partner)

    for dj in range(2):
        for dx in range(nx):
            if dx or dj:
                block = raw.at[r, source(dx), qs[dj]]
                arrived(block, raw_sem, (dj, dx))
                remote(block, block, rawf_sem, (dj, dx), sibling)
    for j in range(2):
        values = [raw[r, k, j].astype(F32) for k in range(nx)]
        total = jnp.sum(functools.reduce(jnp.add, values), axis=1, keepdims=True)
        mean = total / depth
        apart = [v - mean for v in values]
        square = jnp.sum(functools.reduce(jnp.add, [a * a for a in apart]), axis=1, keepdims=True)
        st1[r, z, :, j * half : (j + 1) * half] = columns_to_rows(total, square)
    for dz in range(nz):
        for t, core in enumerate((r, other)):
            if dz or t:
                remote(st1.at[r, z], st1.at[r, z], st1_sem, (t, dz), (core, zs[dz], x, y))
    forward_up(ORDER[0])
    for dx in range(1, nx):
        rows = pl.ds(pl.multiple_of(share(xs[dx]), fc), fc)
        remote(dn_hbm.at[rows, :], wdn.at[:, own], dn_sem, (dx,), (r, z, xs[dx], y))
    forward_up(ORDER[1])
    for dx in range(1, nx):
        arrived(gi.at[source(dx)], g_sem, (0, dx))
        arrived(si.at[source(dx)], g_sem, (1, dx))
    for dj in range(2):
        for dx in range(nx):
            if dx or dj:
                arrived(raw.at[other, source(dx), qs[dj]], rawf_sem, (dj, dx))
    for dz in range(nz):
        for t, core in enumerate((r, other)):
            if dz or t:
                arrived(st1.at[core, zs[nz - dz] if dz else z], st1_sem, (t, dz))
    for i in range(2):
        mean, scale = combine(st1[i], depth)
        for j in range(2):
            part = slice(j * half, (j + 1) * half)
            mean_j, scale_j = row_to_lanes(mean[:, part]), row_to_lanes(scale[:, part])
            for k in range(nx):
                v = (raw[i, k, j].astype(F32) - mean_j) * scale_j * gi[k] + si[k]
                normed[j * nq : (j + 1) * nq, i, :, k * width : (k + 1) * width] = v.astype(BF16).reshape(nq, h, width)

    def partials(blocks, c):
        rows = jnp.concatenate([normed[d].reshape(2 * h, depth) for d in blocks], axis=0)
        both = jnp.dot(rows, wup[c], preferred_element_type=F32)
        return [both[i * 2 * h : (i + 1) * 2 * h] for i in range(len(blocks))]

    def active(c, s):
        return [di for di in range(2) if s < hops(c, di, nz)]

    def target(c, di, s):
        ahead = hops(c, di, nz) - s
        return zs[ahead] if di == 0 else zs[nz - ahead]

    def step_peer(di):
        return (r, zs[1] if di == 0 else zs[nz - 1], x, y)

    def pass_on(c, di, s, value):
        rsb[c, di, s] = value.astype(BF16)
        remote(rsb.at[c, di, s], rrb.at[c, di, s], rs_sem, (c, di, s), step_peer(di))

    forward_up(ORDER[2])
    for c in ORDER:
        up_own[c].wait()
        for dx in range(1, nx):
            arrived(wup.at[c, up_rows(source(dx), 1 - w), :], upf_sem, (c, dx))
        for di, value in zip(active(c, 0), partials([target(c, di, 0) for di in active(c, 0)], c)):
            pass_on(c, di, 0, value)
        if c == ORDER[0]:
            forward_up(ORDER[3])
    for s in range(1, lm + 1):
        for c in ORDER:
            if s < lm:
                blocks = [target(c, di, s) for di in active(c, s)]
                if s == lm - 1:
                    blocks.append(z)
                for slot, value in zip(active(c, s) + [2], partials(blocks, c)):
                    pbuf[c, slot] = value
        for c in ORDER:
            if s < lm:
                for di in active(c, s):
                    arrived(rrb.at[c, di, s - 1], rs_sem, (c, di, s - 1))
                    pass_on(c, di, s, pbuf[c, di] + rrb[c, di, s - 1].astype(F32))
            else:
                value = pbuf[c, 2]
                for di in range(2):
                    last = hops(c, di, nz) - 1
                    arrived(rrb.at[c, di, last], rs_sem, (c, di, last))
                    value = value + rrb[c, di, last].astype(F32)
                hid[c, z] = jnp.square(jnp.maximum(value, 0.0)).astype(BF16)
                for di in range(2):
                    remote(hid.at[c, z], hid.at[c, z], ag_sem, (c, di, 0), step_peer(di))

    def down(ks):
        value = 0.0
        for c in range(NC):
            rows = jnp.concatenate([hid[c, zs[k]] for k in ks], axis=0)
            value += jnp.dot(rows, wdn[c * cw : (c + 1) * cw, :], preferred_element_type=F32)
        for i, k in enumerate(ks):
            o = zs[k]
            bacc[o] = value[i * 2 * h : (i + 1) * 2 * h].reshape(2, h, depth)
            xsend[o] = bacc[o, other].astype(BF16)
            remote(xsend.at[o], xrecv.at[o], x_sem, (k,), sibling)

    def branch(ks):
        for k in ks:
            o = zs[k]
            arrived(xrecv.at[o], x_sem, (k,))
            sb[o] = (bacc[o, r] + xrecv[o].astype(F32)).astype(BF16)
            j, i = lax.div(o, nq), lax.rem(o, nq)
            dj = lax.rem(j + q, 2)
            for dx in range(nx):
                cols = pl.ds(pl.multiple_of(xs[dx] * width, width), width)
                args = (sb.at[o, :, cols], rb.at[dj, dx, i], br_sem, (dj, dx, i), (r, z, xs[dx], y - q + j))
                if dx:
                    remote(*args)
                else:
                    remote_if(dj != 0, *args)

    for s in range(1, lm + 1):
        for c in ORDER:
            for di in range(2):
                length = hops(c, di, nz)
                if s <= length:
                    o = zs[nz - s] if di == 0 else zs[s]
                    arrived(hid.at[c, o], ag_sem, (c, di, s - 1))
                    if s < length:
                        remote(hid.at[c, o], hid.at[c, o], ag_sem, (c, di, s), step_peer(di))
        if s == 1:
            dn_own.wait()
            for dx in range(1, nx):
                arrived(wdn.at[:, pl.ds(pl.multiple_of(source(dx) * width, width), width)], dn_sem, (dx,))
            down((0, 1, nz - 1))
        elif s == 2:
            down((2, nz - 2))
            branch((0, 1, nz - 1))
        elif s < lm:
            down((s, nz - s))
            branch((s - 1, nz - s + 1))
        else:
            down((s,))
            branch((s - 1, nz - s + 1))
            branch((s,))

    blocks = pl.ds(pl.multiple_of(q * nq, nq), nq)
    total = 2.0**0.25 * normed[blocks, r, :, own].astype(F32) + sb[blocks, :, own].astype(F32)
    for dj in range(2):
        for dx in range(nx):
            if dx or dj:
                for i in range(nq):
                    arrived(rb.at[dj, dx, i], br_sem, (dj, dx, i))
                total = total + rb[dj, dx].astype(F32)
    total = total.reshape(half, width)
    tot[r] = total
    remote(tot.at[r], tot.at[r], tot_sem, (), sibling)
    sums = jnp.sum(total, axis=1, keepdims=True)
    apart = total - sums / width
    st2[r, 0] = columns_to_rows(sums, jnp.sum(apart * apart, axis=1, keepdims=True))
    for k in range(nz * nx):
        for t, core in enumerate((r, other)):
            if k or t:
                remote(st2.at[r, 0], st2.at[r, k], st2_sem, (t, k), (core, zs[k // nx], xs[k % nx], y))
    arrived(tot.at[other], tot_sem, ())
    for k in range(nz * nx):
        for t, core in enumerate((r, other)):
            if k or t:
                arrived(st2.at[core, k], st2_sem, (t, k))
    for i in range(2):
        mean, scale = combine(st2[i], width)
        out = (tot[i] - row_to_lanes(mean)) * row_to_lanes(scale) * go[...] + so[...]
        out_ref[i * half : (i + 1) * half, :] = out.astype(BF16)
    for copy, condition in sent:
        if condition is None:
            copy.wait_send()
        else:
            pl.when(condition)(copy.wait_send)


def per_device(nz, nx, residual_in, gain_in, shift_in, up_weight, down_weight, gain_out, shift_out):
    tokens, width = residual_in.shape
    half, nq, depth = tokens // 2, nz // 2, nx * width
    h = half // nq
    fc = up_weight.shape[1] // (2 * nx)
    cw = fc // NC
    dma = pltpu.SemaphoreType.DMA
    row = (1, width)
    return pl.pallas_call(
        functools.partial(kernel, nz, nx),
        out_shape=pltpu.VMEM((tokens, width), BF16),
        in_specs=[pl.BlockSpec(memory_space=pl.ANY)] * 7,
        out_specs=pl.BlockSpec(memory_space=pltpu.VMEM),
        scratch_shapes=[
            pltpu.VMEM((2, nx, 2, half, width), BF16),
            pltpu.VMEM((nx, *row), F32),
            pltpu.VMEM((nx, *row), F32),
            pltpu.VMEM(row, F32),
            pltpu.VMEM(row, F32),
            pltpu.VMEM((NC, depth, cw), BF16),
            pltpu.VMEM((fc, depth), BF16),
            pltpu.VMEM((2, nz, 2, 2 * half), F32),
            pltpu.VMEM((nz, 2, h, depth), BF16),
            pltpu.VMEM((NC, 3, 2 * h, cw), F32),
            pltpu.VMEM((NC, 2, nq, 2 * h, cw), BF16),
            pltpu.VMEM((NC, 2, nq, 2 * h, cw), BF16),
            pltpu.VMEM((NC, nz, 2 * h, cw), BF16),
            pltpu.VMEM((nz, 2, h, depth), F32),
            pltpu.VMEM((nz, h, depth), BF16),
            pltpu.VMEM((nz, h, depth), BF16),
            pltpu.VMEM((nz, h, depth), BF16),
            pltpu.VMEM((2, nx, nq, h, width), BF16),
            pltpu.VMEM((2, nz * nx, 2, half), F32),
            pltpu.VMEM((2, half, width), F32),
            dma((7 + NC,)),
            dma((2, 2, nx)),
            dma((2, 2, nx)),
            dma((2, 2, nx)),
            dma((2, NC, nx)),
            dma((2, NC, nx)),
            dma((2, nx)),
            dma((2, 2, nz)),
            dma((2, NC, 2, nq)),
            dma((2, NC, 2, nq)),
            dma((2, nz)),
            dma((2, 2, nx, nq)),
            dma((2, 2, nz * nx)),
            dma((2,)),
        ],
        compiler_params=pltpu.CompilerParams(collective_id=0, has_side_effects=True),
    )(
        residual_in, gain_in.reshape(row), shift_in.reshape(row), up_weight, down_weight,
        gain_out.reshape(row), shift_out.reshape(row),
    )


def solution(mesh):
    nz, nx = 8, 4
    split = Mesh(
        mesh.devices.reshape(mesh.shape["ra"], nz, nx, mesh.shape["dp"]), ("ra", "cb_0", "cb_1", "dp")
    )
    placed = (P("dp", CB), P(CB), P(CB), P(CB, "ra"), P("ra", CB), P(CB), P(CB))
    return jax.shard_map(
        functools.partial(per_device, nz, nx), mesh=split, in_specs=placed, out_specs=P("dp", CB), check_vma=False
    )
```

```python
import functools

import jax
import jax.numpy as jnp
from jax import lax
from jax.experimental import pallas as pl
from jax.experimental.pallas import tpu as pltpu
from jax.sharding import Mesh
from jax.sharding import PartitionSpec as P

CB = ("cb_0", "cb_1")
MESH = pl.DeviceIdType.MESH
NC = 4
ORDER = (0, 2, 1, 3)
FORWARDED = ORDER[:3]
FAR = (4, 3, 5, 2, 6, 1, 7, 0)
EPS = 1e-05
F32 = jnp.float32
BF16 = jnp.bfloat16


def hops(c, di, nz):
    return nz // 2 if (c < NC // 2) == (di == 0) else nz // 2 - 1


def columns_to_rows(a, b):
    n = a.shape[0]
    lane = lax.broadcasted_iota(jnp.int32, (n, 128), 1)
    both = jnp.where(lane == 0, a, jnp.where(lane == 1, b, 0.0))
    return both.T[0:2, :]


def row_to_lanes(row):
    return jnp.broadcast_to(row, (128, row.shape[1])).T


def combine(stats, count):
    sums, squares = stats[:, 0, :], stats[:, 1, :]
    parts = stats.shape[0]
    mean = jnp.sum(sums, axis=0, keepdims=True) / (parts * count)
    apart = sums / count - mean
    total = jnp.sum(squares, axis=0, keepdims=True) + count * jnp.sum(apart * apart, axis=0, keepdims=True)
    return mean, lax.rsqrt(total / (parts * count) + EPS)


def kernel(
    nz, nx, res_hbm, gi_hbm, si_hbm, up_hbm, dn_hbm, go_hbm, so_hbm, out_ref,
    raw, gi, si, go, so, wup, wdn, st1, normed, pbuf, rsb, rrb, hid, bacc, xsend, xrecv, sb, rb, st2, tot,
    local_sem, send_sem, raw_sem, up_sem, one_sem, ring_sem, x_sem,
):
    half = res_hbm.shape[0] // 2
    width = res_hbm.shape[1]
    nq = nz // 2
    h = half // nq
    depth = nx * width
    fc = wdn.shape[0]
    cw = fc // NC
    lm = nz // 2

    r = lax.axis_index("ra")
    z = lax.axis_index("cb_0")
    x = lax.axis_index("cb_1")
    y = lax.axis_index("dp")
    q = lax.rem(y, 2)
    pf = lax.rem(lax.div(y + 1, 2), 2)
    w = lax.div(y, 2)
    yw = 3 - y
    other = 1 - r
    xs = [lax.rem(x + k, nx) for k in range(nx)]
    zs = [lax.rem(z + k, nz) for k in range(nz)]
    ys = [y, y + 1 - 2 * q]
    qs = [q, 1 - q]
    sibling = (other, z, x, y)
    partner = (r, z, x, yw)

    pairs = [(dj, dx) for dx in (2, 1, 3, 0) for dj in (1, 0) if dx or dj]

    def source(dx):
        return xs[nx - dx] if dx else x

    barrier = pltpu.get_barrier_semaphore()
    greeted = [sibling, partner]
    greeted += [(r, z, xs[dx], ys[dj]) for dj in range(2) for dx in range(nx) if dx or dj]
    greeted += [(c, zs[dz], x, y) for dz in range(1, nz) for c in (r, other)]
    for peer in greeted:
        pl.semaphore_signal(barrier, inc=1, device_id=peer, device_id_type=MESH)

    own = pl.ds(pl.multiple_of(x * width, width), width)
    first = [
        pltpu.make_async_copy(res_hbm.at[0:half, :], raw.at[0, x, q], local_sem.at[0]),
        pltpu.make_async_copy(res_hbm.at[half : 2 * half, :], raw.at[1, x, q], local_sem.at[0]),
        pltpu.make_async_copy(gi_hbm, gi.at[x], local_sem.at[1]),
        pltpu.make_async_copy(si_hbm, si.at[x], local_sem.at[1]),
        pltpu.make_async_copy(go_hbm, go, local_sem.at[1]),
        pltpu.make_async_copy(so_hbm, so, local_sem.at[1]),
    ]
    for copy in first:
        copy.start()

    def share(xd):
        return (xd * 2 + pf) * fc

    for c in range(NC):
        cols = pl.ds(pl.multiple_of(share(x) + c * cw, cw), cw)
        pltpu.make_async_copy(up_hbm.at[:, cols], wup.at[c, own, :], local_sem.at[2]).start()
    rows = pl.ds(pl.multiple_of(share(x), fc), fc)
    pltpu.make_async_copy(dn_hbm.at[rows, :], wdn.at[:, own], local_sem.at[2]).start()

    def remote(src, dst, group, recv, peer):
        copy = pltpu.make_async_remote_copy(
            src_ref=src, dst_ref=dst, send_sem=send_sem.at[group], recv_sem=recv, device_id=peer, device_id_type=MESH
        )
        copy.start()

    def arrived(ref, sem):
        pltpu.make_async_copy(ref, ref, sem).wait()

    arrived(hid.at[0:2], local_sem.at[0])
    arrived(gi, local_sem.at[1])
    pl.semaphore_wait(barrier, len(greeted))

    hw = width // 2

    def up_rows(xd, part):
        return pl.ds(pl.multiple_of(xd * width + part * hw, hw), hw)

    for place, (dj, dx) in enumerate(pairs):
        remote(raw.at[r, x, q], raw.at[r, x, q], 0, raw_sem.at[place], (r, z, xs[dx], ys[dj]))
    for dx in range(1, nx):
        peer = (r, z, xs[dx], y)
        remote(gi.at[x], gi.at[x], 1, one_sem.at[0], peer)
        remote(si.at[x], si.at[x], 1, one_sem.at[1], peer)
    for c in ORDER:
        for dx in range(1, nx):
            cols = pl.ds(pl.multiple_of(share(xs[dx]) + c * cw, cw), cw)
            for part in (w,) if c in FORWARDED else (w, 1 - w):
                rows = pl.ds(pl.multiple_of(part * hw, hw), hw)
                remote(up_hbm.at[rows, cols], wup.at[c, up_rows(x, part), :], 2, up_sem.at[0, c], (r, z, xs[dx], y))

    def forward_up(c):
        arrived(hid.at[0 : nx - 1], up_sem.at[0, c])
        for dx in range(1, nx):
            block = wup.at[c, up_rows(xs[dx], w), :]
            remote(block, block, 3, up_sem.at[1, c], partner)

    for place, (dj, dx) in enumerate(pairs):
        block = raw.at[r, source(dx), qs[dj]]
        arrived(block, raw_sem.at[place])
        remote(block, block, 0, one_sem.at[2], sibling)
    for j in range(2):
        values = [raw[r, k, j].astype(F32) for k in range(nx)]
        total = jnp.sum(functools.reduce(jnp.add, values), axis=1, keepdims=True)
        mean = total / depth
        apart = [v - mean for v in values]
        square = jnp.sum(functools.reduce(jnp.add, [a * a for a in apart]), axis=1, keepdims=True)
        st1[r * nz + z, :, j * half : (j + 1) * half] = columns_to_rows(total, square)
    st1_own = st1.at[r * nz + z]
    for dz in FAR:
        for t, core in enumerate((r, other)):
            if dz or t:
                remote(st1_own, st1_own, 1, one_sem.at[3], (core, zs[dz], x, y))
    forward_up(ORDER[0])
    forward_up(ORDER[1])
    arrived(gi.at[1:nx], one_sem.at[0])
    arrived(si.at[1:nx], one_sem.at[1])
    forward_up(ORDER[2])
    arrived(hid.at[0 : len(pairs)], one_sem.at[2])
    arrived(st1.at[1 : 2 * nz], one_sem.at[3])
    for i in range(2):
        mean, scale = combine(st1[i * nz : (i + 1) * nz], depth)
        for j in range(2):
            part = slice(j * half, (j + 1) * half)
            mean_j, scale_j = row_to_lanes(mean[:, part]), row_to_lanes(scale[:, part])
            for k in range(nx):
                v = (raw[i, k, j].astype(F32) - mean_j) * scale_j * gi[k] + si[k]
                normed[j * nq : (j + 1) * nq, i, :, k * width : (k + 1) * width] = v.astype(BF16).reshape(nq, h, width)

    def partials(blocks, c):
        rows = jnp.concatenate([normed[d].reshape(2 * h, depth) for d in blocks], axis=0)
        both = jnp.dot(rows, wup[c], preferred_element_type=F32)
        return [both[i * 2 * h : (i + 1) * 2 * h] for i in range(len(blocks))]

    def active(c, s):
        return [di for di in range(2) if s < hops(c, di, nz)]

    def target(c, di, s):
        ahead = hops(c, di, nz) - s
        return zs[ahead] if di == 0 else zs[nz - ahead]

    def step_peer(di):
        return (r, zs[1] if di == 0 else zs[nz - 1], x, y)

    def pass_on(c, di, s, value):
        rsb[c, s, di] = value.astype(BF16)
        remote(rsb.at[c, s, di], rrb.at[c, s, di], 4, ring_sem.at[0, c, s], step_peer(di))

    def spread(c, di, s):
        block = hid.at[c * nz + (zs[nz - s if s else 0] if di == 0 else zs[s])]
        remote(block, block, 5, ring_sem.at[1, c, s], step_peer(di))

    arrived(hid.at[0 : 2 * NC + 2 * NC], local_sem.at[2])
    for c in ORDER:
        if c in FORWARDED:
            arrived(hid.at[0 : nx - 1], up_sem.at[1, c])
        else:
            arrived(hid.at[0 : 2 * (nx - 1)], up_sem.at[0, c])
        for di, value in zip(active(c, 0), partials([target(c, di, 0) for di in active(c, 0)], c)):
            pass_on(c, di, 0, value)
    for dx in range(1, nx):
        rows = pl.ds(pl.multiple_of(share(xs[dx]), fc), fc)
        remote(dn_hbm.at[rows, :], wdn.at[:, own], 6, one_sem.at[4], (r, z, xs[dx], y))
    for s in range(1, lm + 1):
        for c in ORDER:
            if s < lm:
                blocks = [target(c, di, s) for di in active(c, s)]
                if s == lm - 1:
                    blocks.append(z)
                for slot, value in zip(active(c, s) + [2], partials(blocks, c)):
                    pbuf[c, slot] = value
        for c in ORDER:
            arrived(rrb.at[c, 0, 0 : len(active(c, s - 1))], ring_sem.at[0, c, s - 1])
            if s < lm:
                for di in active(c, s):
                    pass_on(c, di, s, pbuf[c, di] + rrb[c, s - 1, di].astype(F32))
            else:
                value = pbuf[c, 2]
                for di in range(2):
                    value = value + rrb[c, hops(c, di, nz) - 1, di].astype(F32)
                hid[c * nz + z] = jnp.square(jnp.maximum(value, 0.0)).astype(BF16)
                for di in range(2):
                    spread(c, di, 0)

    def down(ks, stage):
        value = 0.0
        for c in range(NC):
            rows = jnp.concatenate([hid[c * nz + zs[k]] for k in ks], axis=0)
            value += jnp.dot(rows, wdn[c * cw : (c + 1) * cw, :], preferred_element_type=F32)
        for i, k in enumerate(ks):
            o = zs[k]
            bacc[o] = value[i * 2 * h : (i + 1) * 2 * h].reshape(2, h, depth)
            xsend[o] = bacc[o, other].astype(BF16)
            remote(xsend.at[o], xrecv.at[o], 0, x_sem.at[stage], sibling)

    def branch(ks, stage):
        arrived(xrecv.at[0 : len(ks)], x_sem.at[stage])
        for k in ks:
            o = zs[k]
            sb[o] = (bacc[o, r] + xrecv[o].astype(F32)).astype(BF16)
            j, i = lax.div(o, nq), lax.rem(o, nq)
            dj = lax.rem(j + q, 2)
            for dx in range(nx):
                cols = pl.ds(pl.multiple_of(xs[dx] * width, width), width)
                send = functools.partial(
                    remote, sb.at[o, :, cols], rb.at[dj, dx, i], 7, one_sem.at[5], (r, z, xs[dx], y - q + j)
                )
                if dx:
                    send()
                else:
                    pl.when(dj != 0)(send)

    stages = [(0, 1, nz - 1)] + [(k, nz - k) for k in range(2, lm)] + [(lm,)]
    for s in range(1, lm + 1):
        for c in ORDER:
            arrived(hid.at[0 : len(active(c, s - 1))], ring_sem.at[1, c, s - 1])
            for di in active(c, s):
                spread(c, di, s)
        if s == 1:
            arrived(wdn.at[0 : (nx - 1) * fc // nx, :], one_sem.at[4])
        down(stages[s - 1], s - 1)
        if s > 1:
            branch(stages[s - 2], s - 2)
    branch(stages[lm - 1], lm - 1)

    blocks = pl.ds(pl.multiple_of(q * nq, nq), nq)
    total = 2.0**0.25 * normed[blocks, r, :, own].astype(F32) + sb[blocks, :, own].astype(F32)
    arrived(hid.at[0 : len(pairs)], one_sem.at[5])
    for dj, dx in pairs:
        total = total + rb[dj, dx].astype(F32)
    total = total.reshape(half, width)
    tot[r] = total
    remote(tot.at[r], tot.at[r], 0, one_sem.at[6], sibling)
    sums = jnp.sum(total, axis=1, keepdims=True)
    apart = total - sums / width
    st2[r * nz * nx] = columns_to_rows(sums, jnp.sum(apart * apart, axis=1, keepdims=True))
    for dz in FAR:
        for dx in range(nx):
            k = dz * nx + dx
            for t, core in enumerate((r, other)):
                if k or t:
                    remote(st2.at[r * nz * nx], st2.at[r * nz * nx + k], 1, one_sem.at[7], (core, zs[dz], xs[dx], y))
    arrived(tot.at[0], one_sem.at[6])
    arrived(st2.at[1 : 2 * nz * nx], one_sem.at[7])
    for i in range(2):
        mean, scale = combine(st2[i * nz * nx : (i + 1) * nz * nx], width)
        out = (tot[i] - row_to_lanes(mean)) * row_to_lanes(scale) * go[...] + so[...]
        out_ref[i * half : (i + 1) * half, :] = out.astype(BF16)
    for group, units in enumerate((
        2 * len(pairs) + nz + 2, 0, (nx - 1) * (NC + 1), (nx - 1) * (NC - 1), len(pairs) * NC, len(pairs) * NC,
        (nx - 1) * nz, len(pairs),
    )):
        if units:
            arrived(hid.at[0:units], send_sem.at[group])
    arrived(hid.at[0:3], send_sem.at[1])


def per_device(nz, nx, residual_in, gain_in, shift_in, up_weight, down_weight, gain_out, shift_out):
    tokens, width = residual_in.shape
    half, nq, depth = tokens // 2, nz // 2, nx * width
    h = half // nq
    fc = up_weight.shape[1] // (2 * nx)
    cw = fc // NC
    dma = pltpu.SemaphoreType.DMA
    row = (1, width)
    return pl.pallas_call(
        functools.partial(kernel, nz, nx),
        out_shape=pltpu.VMEM((tokens, width), BF16),
        in_specs=[pl.BlockSpec(memory_space=pl.ANY)] * 7,
        out_specs=pl.BlockSpec(memory_space=pltpu.VMEM),
        scratch_shapes=[
            pltpu.VMEM((2, nx, 2, half, width), BF16),
            pltpu.VMEM((nx, *row), F32),
            pltpu.VMEM((nx, *row), F32),
            pltpu.VMEM(row, F32),
            pltpu.VMEM(row, F32),
            pltpu.VMEM((NC, depth, cw), BF16),
            pltpu.VMEM((fc, depth), BF16),
            pltpu.VMEM((2 * nz, 2, 2 * half), F32),
            pltpu.VMEM((nz, 2, h, depth), BF16),
            pltpu.VMEM((NC, 3, 2 * h, cw), F32),
            pltpu.VMEM((NC, nq, 2, 2 * h, cw), BF16),
            pltpu.VMEM((NC, nq, 2, 2 * h, cw), BF16),
            pltpu.VMEM((NC * nz, 2 * h, cw), BF16),
            pltpu.VMEM((nz, 2, h, depth), F32),
            pltpu.VMEM((nz, h, depth), BF16),
            pltpu.VMEM((nz, h, depth), BF16),
            pltpu.VMEM((nz, h, depth), BF16),
            pltpu.VMEM((2, nx, nq, h, width), BF16),
            pltpu.VMEM((2 * nz * nx, 2, half), F32),
            pltpu.VMEM((2, half, width), F32),
            dma((3,)),
            dma((8,)),
            dma((2 * nx - 1,)),
            dma((2, NC)),
            dma((8,)),
            dma((2, NC, nq)),
            dma((nq,)),
        ],
        compiler_params=pltpu.CompilerParams(collective_id=0, has_side_effects=True),
    )(
        residual_in, gain_in.reshape(row), shift_in.reshape(row), up_weight, down_weight,
        gain_out.reshape(row), shift_out.reshape(row),
    )


def solution(mesh):
    nz, nx = 8, 4
    split = Mesh(
        mesh.devices.reshape(mesh.shape["ra"], nz, nx, mesh.shape["dp"]), ("ra", "cb_0", "cb_1", "dp")
    )
    placed = (P("dp", CB), P(CB), P(CB), P(CB, "ra"), P("ra", CB), P(CB), P(CB))
    return jax.shard_map(
        functools.partial(per_device, nz, nx), mesh=split, in_specs=placed, out_specs=P("dp", CB), check_vma=False
    )
```

```python
import functools

import jax
import jax.numpy as jnp
from jax import lax
from jax.experimental import pallas as pl
from jax.experimental.pallas import tpu as pltpu
from jax.sharding import Mesh
from jax.sharding import PartitionSpec as P

CB = ("cb_0", "cb_1")
MESH = pl.DeviceIdType.MESH
NC = 8
ORDER = (4, 0, 5, 1, 6, 2, 7, 3)
FORWARDED = ORDER[:6]
FAR = (4, 3, 5, 2, 6, 1, 7, 0)
MAIN, HELPER = 1, 0
EPS = 1e-05
F32 = jnp.float32
BF16 = jnp.bfloat16


def hops(c, di, nz):
    return nz // 2 if (c < NC // 2) == (di == 0) else nz // 2 - 1


def columns_to_rows(a, b):
    n = a.shape[0]
    lane = lax.broadcasted_iota(jnp.int32, (n, 128), 1)
    both = jnp.where(lane == 0, a, jnp.where(lane == 1, b, 0.0))
    return both.T[0:2, :]


def row_to_lanes(row):
    return jnp.broadcast_to(row, (128, row.shape[1])).T


def combine(stats, count):
    sums, squares = stats[:, 0, :], stats[:, 1, :]
    parts = stats.shape[0]
    mean = jnp.sum(sums, axis=0, keepdims=True) / (parts * count)
    apart = sums / count - mean
    total = jnp.sum(squares, axis=0, keepdims=True) + count * jnp.sum(apart * apart, axis=0, keepdims=True)
    return mean, lax.rsqrt(total / (parts * count) + EPS)


def kernel(
    nz, nx, res_hbm, gi_hbm, si_hbm, up_hbm, dn_hbm, go_hbm, so_hbm, out_ref,
    raw, gi, si, go, so, wup, wdn, st1, normed, pbuf, rsb, rrb, hid, acc, sb, rb, st2, tot,
    local_sem, send_sem, up_sem, one_sem, ring_sem,
):
    tokens, width = res_hbm.shape
    nq = nz // 2
    rows = tokens // nq
    depth = nx * width
    fc = wdn.shape[0]
    fh = fc // 2
    cw = fc // NC
    lm = nz // 2
    hw = width // 2

    r = lax.axis_index("ra")
    z = lax.axis_index("cb_0")
    x = lax.axis_index("cb_1")
    y = lax.axis_index("dp")
    q = lax.rem(y, 2)
    pf = lax.rem(lax.div(y + 1, 2), 2)
    w = lax.div(y, 2)
    yw = 3 - y
    xs = [lax.rem(x + k, nx) for k in range(nx)]
    zs = [lax.rem(z + k, nz) for k in range(nz)]
    ys = [y, y + 1 - 2 * q]
    qs = [q, 1 - q]
    pairs = [(dj, dx) for dx in (2, 1, 3, 0) for dj in (1, 0) if dx or dj]
    own = pl.ds(pl.multiple_of(x * width, width), width)
    unit = hid.at

    def at(core, dz=0, dx=0):
        return (core, zs[dz], xs[dx], y)

    def enter(peers):
        barrier = pltpu.get_barrier_semaphore()
        for peer in peers:
            pl.semaphore_signal(barrier, inc=1, device_id=peer, device_id_type=MESH)
        return lambda: pl.semaphore_wait(barrier, len(peers))

    def remote(src, dst, group, recv, peer):
        copy = pltpu.make_async_remote_copy(
            src_ref=src, dst_ref=dst, send_sem=send_sem.at[group], recv_sem=recv, device_id=peer, device_id_type=MESH
        )
        copy.start()

    def arrived(ref, sem):
        pltpu.make_async_copy(ref, ref, sem).wait()

    def share(xd):
        return pl.multiple_of((xd * 2 + pf) * fh, fh)

    def up_cols(c, xd):
        return pl.ds(pl.multiple_of(share(xd) + c % (NC // 2) * cw, cw), cw)

    def up_rows(xd, part):
        return pl.ds(pl.multiple_of(xd * width + part * hw, hw), hw)

    def dn_rows(core):
        return pl.ds(core * fh, fh)

    def send_up(core):
        for c in ORDER:
            if c // (NC // 2) == core:
                for dx in (2, 1, 3):
                    if c in FORWARDED:
                        part = pl.ds(pl.multiple_of(w * hw, hw), hw)
                        dst = wup.at[c, up_rows(x, w), :]
                        remote(up_hbm.at[part, up_cols(c, xs[dx])], dst, 2, up_sem.at[0, c], at(HELPER, 0, dx))
                    else:
                        dst = wup.at[c, own, :]
                        remote(up_hbm.at[:, up_cols(c, xs[dx])], dst, 2, up_sem.at[1, c], at(MAIN, 0, dx))
                if core == HELPER:
                    remote(up_hbm.at[:, up_cols(c, x)], wup.at[c, own, :], 2, up_sem.at[1, c], at(MAIN))

    def send_down(core):
        for dx in (2, 1, 3):
            src = dn_hbm.at[pl.ds(share(xs[dx]), fh), :]
            remote(src, wdn.at[dn_rows(core), own], 6, one_sem.at[4], at(MAIN, 0, dx))

    def finish():
        mean, scale = combine(st2[0 : nz * nx], width)
        out = (tot[...] - row_to_lanes(mean)) * row_to_lanes(scale) * go[...] + so[...]
        out_ref[...] = out.astype(BF16)

    def helper():
        greeted = enter([(MAIN, z, x, yw), at(MAIN)] + [at(core, 0, dx) for dx in range(1, nx) for core in (0, 1)])
        pltpu.make_async_copy(go_hbm, go, local_sem.at[1]).start()
        pltpu.make_async_copy(so_hbm, so, local_sem.at[1]).start()
        greeted()
        send_up(HELPER)
        for c in FORWARDED:
            arrived(unit[0 : nx - 1], up_sem.at[0, c])
            for dx in range(1, nx):
                block = wup.at[c, up_rows(xs[dx], w), :]
                remote(block, block, 3, up_sem.at[1, c], (MAIN, z, x, yw))
            for dx in range(1, nx):
                block = wup.at[c, up_rows(xs[dx], w), :]
                remote(block, block, 3, up_sem.at[1, c], at(MAIN))
        send_down(HELPER)
        remote(dn_hbm.at[pl.ds(share(x), fh), :], wdn.at[dn_rows(HELPER), own], 6, one_sem.at[4], at(MAIN))
        arrived(gi.at[0:2], local_sem.at[1])
        arrived(unit[0 : (nx - 1) * (NC // 2 + 1) + NC], send_sem.at[2])
        arrived(unit[0 : 2 * (nx - 1) * len(FORWARDED)], send_sem.at[3])
        arrived(unit[0 : nx * NC], send_sem.at[6])
        arrived(unit[0:4], one_sem.at[6])
        arrived(st2.at[0 : nz * nx], one_sem.at[7])
        finish()

    def main():
        greeted = enter(
            [(MAIN, z, xs[dx], ys[dj]) for dj, dx in pairs] + [at(MAIN, dz) for dz in range(1, nz)]
            + [at(HELPER, 0, dx) for dx in range(nx)] + [(HELPER, z, x, yw)]
        )
        pltpu.make_async_copy(res_hbm, raw.at[x, q], local_sem.at[0]).start()
        for src, dst in ((gi_hbm, gi.at[x]), (si_hbm, si.at[x]), (go_hbm, go), (so_hbm, so)):
            pltpu.make_async_copy(src, dst, local_sem.at[1]).start()
        for c in range(NC // 2, NC):
            pltpu.make_async_copy(up_hbm.at[:, up_cols(c, x)], wup.at[c, own, :], local_sem.at[2]).start()
        src = dn_hbm.at[pl.ds(share(x), fh), :]
        pltpu.make_async_copy(src, wdn.at[dn_rows(MAIN), own], local_sem.at[2]).start()
        arrived(unit[0:2], local_sem.at[0])
        arrived(gi, local_sem.at[1])
        greeted()

        for dj, dx in pairs:
            remote(raw.at[x, q], raw.at[x, q], 0, one_sem.at[2 + dj], (MAIN, z, xs[dx], ys[dj]))
        for dx in range(1, nx):
            remote(gi.at[x], gi.at[x], 1, one_sem.at[0], at(MAIN, 0, dx))
            remote(si.at[x], si.at[x], 8, one_sem.at[1], at(MAIN, 0, dx))
        send_up(MAIN)

        for dj in range(2):
            arrived(unit[0 : 2 * (nx - 1 + dj)], one_sem.at[2 + dj])
            values = [raw[k, qs[dj]].astype(F32) for k in range(nx)]
            total = jnp.sum(functools.reduce(jnp.add, values), axis=1, keepdims=True)
            mean = total / depth
            apart = [v - mean for v in values]
            square = jnp.sum(functools.reduce(jnp.add, [a * a for a in apart]), axis=1, keepdims=True)
            st1[z, qs[dj]] = columns_to_rows(total, square)
        for dz in FAR[:-1]:
            remote(st1.at[z], st1.at[z], 9, one_sem.at[8], at(MAIN, dz))
        arrived(gi.at[1:nx], one_sem.at[0])
        arrived(si.at[1:nx], one_sem.at[1])
        arrived(st1.at[1:nz], one_sem.at[8])
        for j in range(2):
            mean, scale = combine(st1[:, j], depth)
            mean, scale = row_to_lanes(mean), row_to_lanes(scale)
            for k in range(nx):
                v = (raw[k, j].astype(F32) - mean) * scale * gi[k] + si[k]
                normed[j * nq : (j + 1) * nq, :, k * width : (k + 1) * width] = v.astype(BF16).reshape(nq, rows, width)

        def partials(blocks, c):
            left = jnp.concatenate([normed[d] for d in blocks], axis=0)
            both = jnp.dot(left, wup[c], preferred_element_type=F32)
            return [both[i * rows : (i + 1) * rows] for i in range(len(blocks))]

        def active(c, s):
            return [di for di in range(2) if s < hops(c, di, nz)]

        def target(c, di, s):
            ahead = hops(c, di, nz) - s
            return zs[ahead] if di == 0 else zs[nz - ahead]

        def pass_on(c, di, s, value):
            rsb[c, s, di] = value.astype(BF16)
            remote(rsb.at[c, s, di], rrb.at[c, s, di], 4, ring_sem.at[0, c, s], at(MAIN, 1 if di == 0 else nz - 1))

        def spread(c, di, s):
            block = unit[c * nz + (zs[nz - s if s else 0] if di == 0 else zs[s])]
            remote(block, block, 5, ring_sem.at[1, c, s], at(MAIN, 1 if di == 0 else nz - 1))

        def prepare(c, s):
            blocks = [target(c, di, s) for di in active(c, s)]
            if s == lm - 1:
                blocks.append(z)
            for slot, value in zip(active(c, s) + [2], partials(blocks, c)):
                pbuf[c, slot] = value

        arrived(unit[0 : 2 * NC], local_sem.at[2])
        for c in ORDER:
            arrived(unit[0 : 2 * (nx - 1) + (2 if c < NC // 2 else 0)], up_sem.at[1, c])
            for di, value in zip(active(c, 0), partials([target(c, di, 0) for di in active(c, 0)], c)):
                pass_on(c, di, 0, value)
            prepare(c, 1)
        send_down(MAIN)
        for s in range(1, lm + 1):
            for c in ORDER:
                arrived(rrb.at[c, 0, 0 : len(active(c, s - 1))], ring_sem.at[0, c, s - 1])
                if s < lm:
                    for di in active(c, s):
                        pass_on(c, di, s, pbuf[c, di] + rrb[c, s - 1, di].astype(F32))
                    if s < lm - 1:
                        prepare(c, s + 1)
                else:
                    value = pbuf[c, 2]
                    for di in range(2):
                        value = value + rrb[c, hops(c, di, nz) - 1, di].astype(F32)
                    hid[c * nz + z] = jnp.square(jnp.maximum(value, 0.0)).astype(BF16)
                    for di in range(2):
                        spread(c, di, 0)

        def down(c, ks):
            left = jnp.concatenate([hid[c * nz + zs[k]] for k in ks], axis=0)
            value = jnp.dot(left, wdn[c * cw : (c + 1) * cw, :], preferred_element_type=F32)
            for i, k in enumerate(ks):
                part = value[i * rows : (i + 1) * rows]
                acc[k] = part if c == ORDER[0] else acc[k] + part

        def branch(ks):
            for k in ks:
                o = zs[k]
                sb[o] = acc[k].astype(BF16)
                j, i = lax.div(o, nq), lax.rem(o, nq)
                dj = lax.rem(j + q, 2)
                for dx in (2, 1, 3, 0):
                    cols = pl.ds(pl.multiple_of(xs[dx] * width, width), width)
                    send = functools.partial(
                        remote, sb.at[o, :, cols], rb.at[dj, dx, i], 7, one_sem.at[5], (MAIN, z, xs[dx], y - q + j)
                    )
                    if dx:
                        send()
                    else:
                        pl.when(dj != 0)(send)

        stages = [(0, 1, nz - 1)] + [(k, nz - k) for k in range(2, lm)] + [(lm,)]
        for s in range(1, lm + 1):
            if s == 2:
                arrived(unit[0 : NC * (nx - 1) * 2 + NC], one_sem.at[4])
            for c in ORDER:
                arrived(unit[0 : len(active(c, s - 1))], ring_sem.at[1, c, s - 1])
                for di in active(c, s):
                    spread(c, di, s)
                if s > 1:
                    down(c, stages[s - 2] if s < lm else stages[s - 1])
            if 1 < s < lm:
                branch(stages[s - 2])
            if s == lm - 1:
                for c in ORDER:
                    down(c, stages[s - 1])
                branch(stages[s - 1])
        branch(stages[lm - 1])

        blocks = pl.ds(pl.multiple_of(q * nq, nq), nq)
        total = 2.0**0.25 * normed[blocks, :, own].astype(F32) + sb[blocks, :, own].astype(F32)
        arrived(unit[0 : 2 * len(pairs)], one_sem.at[5])
        for dj, dx in pairs:
            total = total + rb[dj, dx].astype(F32)
        total = total.reshape(tokens, width)
        sums = jnp.sum(total, axis=1, keepdims=True)
        apart = total - sums / width
        st2[0] = columns_to_rows(sums, jnp.sum(apart * apart, axis=1, keepdims=True))
        tot[...] = total
        for core in (MAIN, HELPER):
            for dz in FAR:
                for dx in (2, 1, 3, 0):
                    k = dz * nx + dx
                    if k or core == HELPER:
                        remote(st2.at[0], st2.at[k], 10, one_sem.at[7], at(core, dz, dx))
            if core == MAIN:
                remote(tot, tot, 0, one_sem.at[6], at(HELPER))
        arrived(st2.at[1 : nz * nx], one_sem.at[7])
        finish()

        for group, ref in (
            (0, unit[0 : 2 * len(pairs) + 4]),
            (1, gi.at[1:nx]),
            (8, si.at[1:nx]),
            (2, unit[0 : (nx - 1) * (NC // 2 + 1)]),
            (4, unit[0 : len(pairs) * NC]),
            (5, unit[0 : len(pairs) * NC]),
            (6, unit[0 : (nx - 1) * NC]),
            (7, unit[0 : 2 * len(pairs)]),
            (9, st1.at[1:nz]),
            (10, st2.at[1 : 2 * nz * nx]),
        ):
            arrived(ref, send_sem.at[group])

    pl.when(r == MAIN)(main)
    pl.when(r == HELPER)(helper)


def per_device(nz, nx, residual_in, gain_in, shift_in, up_weight, down_weight, gain_out, shift_out):
    tokens, width = residual_in.shape
    nq, depth = nz // 2, nx * width
    rows = tokens // nq
    fc = up_weight.shape[1] // nx
    cw = fc // NC
    dma = pltpu.SemaphoreType.DMA
    row = (1, width)
    return pl.pallas_call(
        functools.partial(kernel, nz, nx),
        out_shape=pltpu.VMEM((tokens, width), BF16),
        in_specs=[pl.BlockSpec(memory_space=pl.ANY)] * 7,
        out_specs=pl.BlockSpec(memory_space=pltpu.VMEM),
        scratch_shapes=[
            pltpu.VMEM((nx, 2, tokens, width), BF16),
            pltpu.VMEM((nx, *row), F32),
            pltpu.VMEM((nx, *row), F32),
            pltpu.VMEM(row, F32),
            pltpu.VMEM(row, F32),
            pltpu.VMEM((NC, depth, cw), BF16),
            pltpu.VMEM((fc, depth), BF16),
            pltpu.VMEM((nz, 2, 2, tokens), F32),
            pltpu.VMEM((nz, rows, depth), BF16),
            pltpu.VMEM((NC, 3, rows, cw), F32),
            pltpu.VMEM((NC, nq, 2, rows, cw), BF16),
            pltpu.VMEM((NC, nq, 2, rows, cw), BF16),
            pltpu.VMEM((NC * nz, rows, cw), BF16),
            pltpu.VMEM((nz, rows, depth), F32),
            pltpu.VMEM((nz, rows, depth), BF16),
            pltpu.VMEM((2, nx, nq, rows, width), BF16),
            pltpu.VMEM((2 * nz * nx, 2, tokens), F32),
            pltpu.VMEM((tokens, width), F32),
            dma((3,)),
            dma((11,)),
            dma((2, NC)),
            dma((9,)),
            dma((2, NC, nq)),
        ],
        compiler_params=pltpu.CompilerParams(collective_id=0, has_side_effects=True),
    )(
        residual_in, gain_in.reshape(row), shift_in.reshape(row), up_weight, down_weight,
        gain_out.reshape(row), shift_out.reshape(row),
    )


def solution(mesh):
    nz, nx = 8, 4
    split = Mesh(
        mesh.devices.reshape(mesh.shape["ra"], nz, nx, mesh.shape["dp"]), ("ra", "cb_0", "cb_1", "dp")
    )
    placed = (P("dp", CB), P(CB), P(CB), P(CB, "ra"), P("ra", CB), P(CB), P(CB))
    return jax.shard_map(
        functools.partial(per_device, nz, nx), mesh=split, in_specs=placed, out_specs=P("dp", CB), check_vma=False
    )
```

```python
import functools

import jax
import jax.numpy as jnp
from jax import lax
from jax.experimental import pallas as pl
from jax.experimental.pallas import tpu as pltpu
from jax.sharding import Mesh
from jax.sharding import PartitionSpec as P

CB = ("cb_0", "cb_1")
MESH = pl.DeviceIdType.MESH
NC = 8
ORDER = (0, 1, 2, 3, 4, 5, 6, 7)
FORWARDED = (0, 1, 2, 4, 5)
FAR = (4, 3, 5, 2, 6, 1, 7, 0)
MAIN, HELPER = 1, 0
EPS = 1e-05
F32 = jnp.float32
BF16 = jnp.bfloat16


def hops(c, di, nz):
    return nz // 2 - (ORDER.index(c) + di) % 2


def columns_to_rows(a, b):
    n = a.shape[0]
    lane = lax.broadcasted_iota(jnp.int32, (n, 128), 1)
    both = jnp.where(lane == 0, a, jnp.where(lane == 1, b, 0.0))
    return both.T[0:2, :]


def row_to_lanes(row):
    return jnp.broadcast_to(row, (128, row.shape[1])).T


def combine(stats, count):
    sums, squares = stats[:, 0, :], stats[:, 1, :]
    parts = stats.shape[0]
    mean = jnp.sum(sums, axis=0, keepdims=True) / (parts * count)
    apart = sums / count - mean
    total = jnp.sum(squares, axis=0, keepdims=True) + count * jnp.sum(apart * apart, axis=0, keepdims=True)
    return mean, lax.rsqrt(total / (parts * count) + EPS)


def kernel(
    nz, nx, res_hbm, gi_hbm, si_hbm, up_hbm, dn_hbm, go_hbm, so_hbm, out_ref,
    raw, gi, si, go, so, wup, wdn, st1, normed, pbuf, rsb, rrb, hid, acc, sb, rb, st2, tot,
    local_sem, send_sem, up_sem, one_sem, ring_sem, reach_sem,
):
    tokens, width = res_hbm.shape
    nq = nz // 2
    rows = tokens // nq
    depth = nx * width
    fc = wdn.shape[0]
    fh = fc // 2
    cw = fc // NC
    lm = nz // 2
    hw = width // 2

    r = lax.axis_index("ra")
    z = lax.axis_index("cb_0")
    x = lax.axis_index("cb_1")
    y = lax.axis_index("dp")
    q = lax.rem(y, 2)
    pf = lax.rem(lax.div(y + 1, 2), 2)
    w = lax.div(y, 2)
    yw = 3 - y
    xs = [lax.rem(x + k, nx) for k in range(nx)]
    zs = [lax.rem(z + k, nz) for k in range(nz)]
    ys = [y, y + 1 - 2 * q]
    qs = [q, 1 - q]
    pairs = [(dj, dx) for dx in (2, 1, 3, 0) for dj in (1, 0) if dx or dj]
    own = pl.ds(pl.multiple_of(x * width, width), width)
    unit = hid.at

    def at(core, dz=0, dx=0):
        return (core, zs[dz], xs[dx], y)

    def enter(peers):
        barrier = pltpu.get_barrier_semaphore()
        for peer in peers:
            pl.semaphore_signal(barrier, inc=1, device_id=peer, device_id_type=MESH)
        return lambda: pl.semaphore_wait(barrier, len(peers))

    def remote(src, dst, group, recv, peer):
        copy = pltpu.make_async_remote_copy(
            src_ref=src, dst_ref=dst, send_sem=send_sem.at[group], recv_sem=recv, device_id=peer, device_id_type=MESH
        )
        copy.start()

    def arrived(ref, sem):
        pltpu.make_async_copy(ref, ref, sem).wait()

    def share(xd):
        return pl.multiple_of((xd * 2 + pf) * fh, fh)

    def up_cols(c, xd):
        return pl.ds(pl.multiple_of(share(xd) + c % (NC // 2) * cw, cw), cw)

    def up_rows(xd, part):
        return pl.ds(pl.multiple_of(xd * width + part * hw, hw), hw)

    def dn_rows(core):
        return pl.ds(core * fh, fh)

    def send_up(core, chunks):
        for c in chunks:
            if c // (NC // 2) == core:
                for dx in (2, 1, 3):
                    if c in FORWARDED:
                        part = pl.ds(pl.multiple_of(w * hw, hw), hw)
                        dst = wup.at[c, up_rows(x, w), :]
                        remote(up_hbm.at[part, up_cols(c, xs[dx])], dst, 2, up_sem.at[0, c], at(HELPER, 0, dx))
                    else:
                        dst = wup.at[c, own, :]
                        remote(up_hbm.at[:, up_cols(c, xs[dx])], dst, 2, up_sem.at[1, c], at(MAIN, 0, dx))
                if core == HELPER:
                    remote(up_hbm.at[:, up_cols(c, x)], wup.at[c, own, :], 2, up_sem.at[1, c], at(MAIN))

    def up_units(core):
        return sum((nx - 1) * (1 if c in FORWARDED else 2) for c in ORDER if c // (NC // 2) == core)

    def send_down(core):
        for dx in (2, 1, 3):
            src = dn_hbm.at[pl.ds(share(xs[dx]), fh), :]
            remote(src, wdn.at[dn_rows(core), own], 6, one_sem.at[4], at(MAIN, 0, dx))

    def finish():
        mean, scale = combine(st2[0 : nz * nx], width)
        out = (tot[...] - row_to_lanes(mean)) * row_to_lanes(scale) * go[...] + so[...]
        out_ref[...] = out.astype(BF16)

    def helper():
        greeted = enter([(MAIN, z, x, yw), at(MAIN)] + [at(core, 0, dx) for dx in range(1, nx) for core in (0, 1)])
        pltpu.make_async_copy(go_hbm, go, local_sem.at[1]).start()
        pltpu.make_async_copy(so_hbm, so, local_sem.at[1]).start()
        greeted()
        send_up(HELPER, FORWARDED)
        for c in FORWARDED:
            arrived(unit[0 : nx - 1], up_sem.at[0, c])
            for dx in range(1, nx):
                block = wup.at[c, up_rows(xs[dx], w), :]
                remote(block, block, 3, up_sem.at[1, c], (MAIN, z, x, yw))
            for dx in range(1, nx):
                block = wup.at[c, up_rows(xs[dx], w), :]
                remote(block, block, 3, up_sem.at[1, c], at(MAIN))
            if c == FORWARDED[1]:
                send_up(HELPER, [c for c in ORDER if c not in FORWARDED])
        send_down(HELPER)
        remote(dn_hbm.at[pl.ds(share(x), fh), :], wdn.at[dn_rows(HELPER), own], 6, one_sem.at[4], at(MAIN))
        arrived(gi.at[0:2], local_sem.at[1])
        arrived(unit[0 : up_units(HELPER) + NC], send_sem.at[2])
        arrived(unit[0 : 2 * (nx - 1) * len(FORWARDED)], send_sem.at[3])
        arrived(unit[0 : nx * NC], send_sem.at[6])
        arrived(unit[0:4], one_sem.at[6])
        arrived(st2.at[0 : nz * nx], one_sem.at[7])
        finish()

    def main():
        greeted = enter(
            [(MAIN, z, xs[dx], ys[dj]) for dj, dx in pairs] + [at(MAIN, dz) for dz in (1, nz - 1)]
            + [at(HELPER, 0, dx) for dx in range(nx)] + [(HELPER, z, x, yw)]
        )
        pltpu.make_async_copy(res_hbm, raw.at[x, q], local_sem.at[0]).start()
        for src, dst in ((gi_hbm, gi.at[x]), (si_hbm, si.at[x]), (go_hbm, go), (so_hbm, so)):
            pltpu.make_async_copy(src, dst, local_sem.at[1]).start()
        for c in range(NC // 2, NC):
            pltpu.make_async_copy(up_hbm.at[:, up_cols(c, x)], wup.at[c, own, :], local_sem.at[2]).start()
        src = dn_hbm.at[pl.ds(share(x), fh), :]
        pltpu.make_async_copy(src, wdn.at[dn_rows(MAIN), own], local_sem.at[2]).start()
        arrived(unit[0:2], local_sem.at[0])
        arrived(gi, local_sem.at[1])
        greeted()

        for dj, dx in pairs:
            remote(raw.at[x, q], raw.at[x, q], 0, one_sem.at[2 + dj], (MAIN, z, xs[dx], ys[dj]))
        for dx in range(1, nx):
            remote(gi.at[x], gi.at[x], 1, one_sem.at[0], at(MAIN, 0, dx))
            remote(si.at[x], si.at[x], 8, one_sem.at[1], at(MAIN, 0, dx))
        send_up(MAIN, ORDER)

        for k in range(lm - 1):
            for dz in (1, nz - 1):
                pl.semaphore_signal(reach_sem.at[k], inc=1, device_id=at(MAIN, dz), device_id_type=MESH)
            pl.semaphore_wait(reach_sem.at[k], 2)

        for dj in range(2):
            arrived(unit[0 : 2 * (nx - 1 + dj)], one_sem.at[2 + dj])
            values = [raw[k, qs[dj]].astype(F32) for k in range(nx)]
            total = jnp.sum(functools.reduce(jnp.add, values), axis=1, keepdims=True)
            mean = total / depth
            apart = [v - mean for v in values]
            square = jnp.sum(functools.reduce(jnp.add, [a * a for a in apart]), axis=1, keepdims=True)
            st1[z, qs[dj]] = columns_to_rows(total, square)
        for dz in FAR[:-1]:
            remote(st1.at[z], st1.at[z], 9, one_sem.at[8], at(MAIN, dz))
        arrived(gi.at[1:nx], one_sem.at[0])
        arrived(si.at[1:nx], one_sem.at[1])
        arrived(st1.at[1:nz], one_sem.at[8])
        for j in range(2):
            mean, scale = combine(st1[:, j], depth)
            mean, scale = row_to_lanes(mean), row_to_lanes(scale)
            for k in range(nx):
                v = (raw[k, j].astype(F32) - mean) * scale * gi[k] + si[k]
                normed[j * nq : (j + 1) * nq, :, k * width : (k + 1) * width] = v.astype(BF16).reshape(nq, rows, width)

        def partials(blocks, c):
            left = jnp.concatenate([normed[d] for d in blocks], axis=0)
            both = jnp.dot(left, wup[c], preferred_element_type=F32)
            return [both[i * rows : (i + 1) * rows] for i in range(len(blocks))]

        def active(c, s):
            return [di for di in range(2) if s < hops(c, di, nz)]

        def target(c, di, s):
            ahead = hops(c, di, nz) - s
            return zs[ahead] if di == 0 else zs[nz - ahead]

        def pass_on(c, di, s, value):
            rsb[c, s, di] = value.astype(BF16)
            remote(rsb.at[c, s, di], rrb.at[c, s, di], 4, ring_sem.at[0, c, s], at(MAIN, 1 if di == 0 else nz - 1))

        def spread(c, di, s):
            block = unit[c * nz + (zs[nz - s if s else 0] if di == 0 else zs[s])]
            remote(block, block, 5, ring_sem.at[1, c, s], at(MAIN, 1 if di == 0 else nz - 1))

        def prepare(c, s):
            blocks = [target(c, di, s) for di in active(c, s)]
            if s == lm - 1:
                blocks.append(z)
            for slot, value in zip(active(c, s) + [2], partials(blocks, c)):
                pbuf[c, slot] = value

        arrived(unit[0 : 2 * NC], local_sem.at[2])
        for c in ORDER:
            arrived(unit[0 : 2 * (nx - 1) + (2 if c < NC // 2 else 0)], up_sem.at[1, c])
            for di, value in zip(active(c, 0), partials([target(c, di, 0) for di in active(c, 0)], c)):
                pass_on(c, di, 0, value)
            prepare(c, 1)
        send_down(MAIN)
        for s in range(1, lm + 1):
            for c in ORDER:
                arrived(rrb.at[c, 0, 0 : len(active(c, s - 1))], ring_sem.at[0, c, s - 1])
                if s < lm:
                    for di in active(c, s):
                        pass_on(c, di, s, pbuf[c, di] + rrb[c, s - 1, di].astype(F32))
                    if s < lm - 1:
                        prepare(c, s + 1)
                else:
                    value = pbuf[c, 2]
                    for di in range(2):
                        value = value + rrb[c, hops(c, di, nz) - 1, di].astype(F32)
                    hid[c * nz + z] = jnp.square(jnp.maximum(value, 0.0)).astype(BF16)
                    for di in range(2):
                        spread(c, di, 0)

        def down(c, ks):
            left = jnp.concatenate([hid[c * nz + zs[k]] for k in ks], axis=0)
            value = jnp.dot(left, wdn[c * cw : (c + 1) * cw, :], preferred_element_type=F32)
            for i, k in enumerate(ks):
                part = value[i * rows : (i + 1) * rows]
                acc[k] = part if c == ORDER[0] else acc[k] + part

        def branch(ks):
            for k in ks:
                o = zs[k]
                sb[o] = acc[k].astype(BF16)
                j, i = lax.div(o, nq), lax.rem(o, nq)
                dj = lax.rem(j + q, 2)
                for dx in (2, 1, 3, 0):
                    cols = pl.ds(pl.multiple_of(xs[dx] * width, width), width)
                    send = functools.partial(
                        remote, sb.at[o, :, cols], rb.at[dj, dx, i], 7, one_sem.at[5], (MAIN, z, xs[dx], y - q + j)
                    )
                    if dx:
                        send()
                    else:
                        pl.when(dj != 0)(send)

        stages = [(0, 1, nz - 1)] + [(k, nz - k) for k in range(2, lm)] + [(lm,)]
        for s in range(1, lm + 1):
            if s == 2:
                arrived(unit[0 : NC * (nx - 1) * 2 + NC], one_sem.at[4])
            for c in ORDER:
                arrived(unit[0 : len(active(c, s - 1))], ring_sem.at[1, c, s - 1])
                for di in active(c, s):
                    spread(c, di, s)
                if s > 1:
                    down(c, stages[s - 2] if s < lm else stages[s - 1])
            if 1 < s < lm:
                branch(stages[s - 2])
            if s == lm - 1:
                for c in ORDER:
                    down(c, stages[s - 1])
                branch(stages[s - 1])
        branch(stages[lm - 1])

        blocks = pl.ds(pl.multiple_of(q * nq, nq), nq)
        total = 2.0**0.25 * normed[blocks, :, own].astype(F32) + sb[blocks, :, own].astype(F32)
        arrived(unit[0 : 2 * len(pairs)], one_sem.at[5])
        for dj, dx in pairs:
            total = total + rb[dj, dx].astype(F32)
        total = total.reshape(tokens, width)
        sums = jnp.sum(total, axis=1, keepdims=True)
        apart = total - sums / width
        st2[0] = columns_to_rows(sums, jnp.sum(apart * apart, axis=1, keepdims=True))
        tot[...] = total
        for core in (MAIN, HELPER):
            for dz in FAR:
                for dx in (2, 1, 3, 0):
                    k = dz * nx + dx
                    if k or core == HELPER:
                        remote(st2.at[0], st2.at[k], 10, one_sem.at[7], at(core, dz, dx))
            if core == MAIN:
                remote(tot, tot, 0, one_sem.at[6], at(HELPER))
        arrived(st2.at[1 : nz * nx], one_sem.at[7])
        finish()

        for group, ref in (
            (0, unit[0 : 2 * len(pairs) + 4]),
            (1, gi.at[1:nx]),
            (8, si.at[1:nx]),
            (2, unit[0 : up_units(MAIN)]),
            (4, unit[0 : len(pairs) * NC]),
            (5, unit[0 : len(pairs) * NC]),
            (6, unit[0 : (nx - 1) * NC]),
            (7, unit[0 : 2 * len(pairs)]),
            (9, st1.at[1:nz]),
            (10, st2.at[1 : 2 * nz * nx]),
        ):
            arrived(ref, send_sem.at[group])

    pl.when(r == MAIN)(main)
    pl.when(r == HELPER)(helper)


def per_device(nz, nx, residual_in, gain_in, shift_in, up_weight, down_weight, gain_out, shift_out):
    tokens, width = residual_in.shape
    nq, depth = nz // 2, nx * width
    rows = tokens // nq
    fc = up_weight.shape[1] // nx
    cw = fc // NC
    dma = pltpu.SemaphoreType.DMA
    row = (1, width)
    return pl.pallas_call(
        functools.partial(kernel, nz, nx),
        out_shape=pltpu.VMEM((tokens, width), BF16),
        in_specs=[pl.BlockSpec(memory_space=pl.ANY)] * 7,
        out_specs=pl.BlockSpec(memory_space=pltpu.VMEM),
        scratch_shapes=[
            pltpu.VMEM((nx, 2, tokens, width), BF16),
            pltpu.VMEM((nx, *row), F32),
            pltpu.VMEM((nx, *row), F32),
            pltpu.VMEM(row, F32),
            pltpu.VMEM(row, F32),
            pltpu.VMEM((NC, depth, cw), BF16),
            pltpu.VMEM((fc, depth), BF16),
            pltpu.VMEM((nz, 2, 2, tokens), F32),
            pltpu.VMEM((nz, rows, depth), BF16),
            pltpu.VMEM((NC, 3, rows, cw), F32),
            pltpu.VMEM((NC, nq, 2, rows, cw), BF16),
            pltpu.VMEM((NC, nq, 2, rows, cw), BF16),
            pltpu.VMEM((NC * nz, rows, cw), BF16),
            pltpu.VMEM((nz, rows, depth), F32),
            pltpu.VMEM((nz, rows, depth), BF16),
            pltpu.VMEM((2, nx, nq, rows, width), BF16),
            pltpu.VMEM((2 * nz * nx, 2, tokens), F32),
            pltpu.VMEM((tokens, width), F32),
            dma((3,)),
            dma((11,)),
            dma((2, NC)),
            dma((9,)),
            dma((2, NC, nq)),
            pltpu.SemaphoreType.REGULAR((nq - 1,)),
        ],
        compiler_params=pltpu.CompilerParams(collective_id=0, has_side_effects=True),
    )(
        residual_in, gain_in.reshape(row), shift_in.reshape(row), up_weight, down_weight,
        gain_out.reshape(row), shift_out.reshape(row),
    )


def solution(mesh):
    nz, nx = 8, 4
    split = Mesh(
        mesh.devices.reshape(mesh.shape["ra"], nz, nx, mesh.shape["dp"]), ("ra", "cb_0", "cb_1", "dp")
    )
    placed = (P("dp", CB), P(CB), P(CB), P(CB, "ra"), P("ra", CB), P(CB), P(CB))
    return jax.shard_map(
        functools.partial(per_device, nz, nx), mesh=split, in_specs=placed, out_specs=P("dp", CB), check_vma=False
    )
```

```python
import functools

import jax
import jax.numpy as jnp
from jax import lax
from jax.experimental import pallas as pl
from jax.experimental.pallas import tpu as pltpu
from jax.sharding import Mesh
from jax.sharding import PartitionSpec as P

CB = ("cb_0", "cb_1")
MESH = pl.DeviceIdType.MESH
NC = 8
ORDER = (0, 1, 2, 3, 4, 5, 6, 7)
FORWARDED = (0, 1, 2, 4)
EARLY = (0, 1, 2)
FAR = (4, 3, 5, 2, 6, 1, 7, 0)
MAIN, HELPER = 1, 0
EPS = 1e-05
F32 = jnp.float32
BF16 = jnp.bfloat16


def hops(c, di, nz):
    return nz // 2 - (ORDER.index(c) + di) % 2


def columns_to_rows(a, b):
    n = a.shape[0]
    lane = lax.broadcasted_iota(jnp.int32, (n, 128), 1)
    both = jnp.where(lane == 0, a, jnp.where(lane == 1, b, 0.0))
    return both.T[0:2, :]


def row_to_lanes(row):
    return jnp.broadcast_to(row, (128, row.shape[1])).T


def pool(stats, count):
    sums, squares = stats[:, 0, :], stats[:, 1, :]
    total = jnp.sum(sums, axis=0, keepdims=True)
    apart = sums / count - total / (stats.shape[0] * count)
    return total, jnp.sum(squares, axis=0, keepdims=True) + count * jnp.sum(apart * apart, axis=0, keepdims=True)


def combine(stats, count):
    total, square = pool(stats, count)
    whole = stats.shape[0] * count
    return total / whole, lax.rsqrt(square / whole + EPS)


def of_shard(values):
    sums = jnp.sum(values, axis=1, keepdims=True)
    apart = values - sums / values.shape[1]
    return columns_to_rows(sums, jnp.sum(apart * apart, axis=1, keepdims=True))


def kernel(
    nz, nx, res_hbm, gi_hbm, si_hbm, up_hbm, dn_hbm, go_hbm, so_hbm, out_ref,
    raw, gi, si, go, so, wup, wdn, st0, st1, normed, pbuf, rsb, rrb, hid, acc, sb, rb, st2, tot,
    local_sem, send_sem, up_sem, one_sem, ring_sem, reach_sem,
):
    tokens, width = res_hbm.shape
    nq = nz // 2
    rows = tokens // nq
    depth = nx * width
    fc = wdn.shape[0]
    fh = fc // 2
    cw = fc // NC
    lm = nz // 2
    hw = width // 2

    r = lax.axis_index("ra")
    z = lax.axis_index("cb_0")
    x = lax.axis_index("cb_1")
    y = lax.axis_index("dp")
    q = lax.rem(y, 2)
    pf = lax.rem(lax.div(y + 1, 2), 2)
    w = lax.div(y, 2)
    yw = 3 - y
    xs = [lax.rem(x + k, nx) for k in range(nx)]
    zs = [lax.rem(z + k, nz) for k in range(nz)]
    ys = [y, y + 1 - 2 * q]
    qs = [q, 1 - q]
    pairs = [(dj, dx) for dx in (2, 1, 3, 0) for dj in (1, 0) if dx or dj]
    own = pl.ds(pl.multiple_of(x * width, width), width)
    unit = hid.at

    def at(core, dz=0, dx=0):
        return (core, zs[dz], xs[dx], y)

    def enter(peers):
        barrier = pltpu.get_barrier_semaphore()
        for peer in peers:
            pl.semaphore_signal(barrier, inc=1, device_id=peer, device_id_type=MESH)
        return lambda: pl.semaphore_wait(barrier, len(peers))

    def remote(src, dst, group, recv, peer):
        copy = pltpu.make_async_remote_copy(
            src_ref=src, dst_ref=dst, send_sem=send_sem.at[group], recv_sem=recv, device_id=peer, device_id_type=MESH
        )
        copy.start()

    def arrived(ref, sem):
        pltpu.make_async_copy(ref, ref, sem).wait()

    def share(xd):
        return pl.multiple_of((xd * 2 + pf) * fh, fh)

    def up_cols(c, xd):
        return pl.ds(pl.multiple_of(share(xd) + c % (NC // 2) * cw, cw), cw)

    def up_rows(xd, part):
        return pl.ds(pl.multiple_of(xd * width + part * hw, hw), hw)

    def dn_rows(core):
        return pl.ds(core * fh, fh)

    def send_up(core, chunks):
        for c in chunks:
            if c // (NC // 2) == core:
                for dx in (2, 1, 3):
                    if c in FORWARDED:
                        part = pl.ds(pl.multiple_of(w * hw, hw), hw)
                        dst = wup.at[c, up_rows(x, w), :]
                        remote(up_hbm.at[part, up_cols(c, xs[dx])], dst, 2, up_sem.at[0, c], at(HELPER, 0, dx))
                    else:
                        dst = wup.at[c, own, :]
                        remote(up_hbm.at[:, up_cols(c, xs[dx])], dst, 2, up_sem.at[1, c], at(MAIN, 0, dx))
                if core == HELPER:
                    remote(up_hbm.at[:, up_cols(c, x)], wup.at[c, own, :], 2, up_sem.at[1, c], at(MAIN))

    def up_units(core):
        return sum((nx - 1) * (1 if c in FORWARDED else 2) for c in ORDER if c // (NC // 2) == core)

    def send_down(core):
        for dx in (2, 1, 3):
            src = dn_hbm.at[pl.ds(share(xs[dx]), fh), :]
            remote(src, wdn.at[dn_rows(core), own], 6, one_sem.at[4], at(MAIN, 0, dx))

    def finish():
        mean, scale = combine(st2[0 : nz * nx], width)
        out = (tot[...] - row_to_lanes(mean)) * row_to_lanes(scale) * go[...] + so[...]
        out_ref[...] = out.astype(BF16)

    def helper():
        greeted = enter([(MAIN, z, x, yw), at(MAIN)] + [at(core, 0, dx) for dx in range(1, nx) for core in (0, 1)])
        pltpu.make_async_copy(go_hbm, go, local_sem.at[1]).start()
        pltpu.make_async_copy(so_hbm, so, local_sem.at[1]).start()
        greeted()
        send_up(HELPER, EARLY)
        for c in FORWARDED:
            arrived(unit[0 : nx - 1], up_sem.at[0, c])
            for dx in range(1, nx):
                block = wup.at[c, up_rows(xs[dx], w), :]
                remote(block, block, 3, up_sem.at[1, c], (MAIN, z, x, yw))
            for dx in range(1, nx):
                block = wup.at[c, up_rows(xs[dx], w), :]
                remote(block, block, 3, up_sem.at[1, c], at(MAIN))
            if c == FORWARDED[0]:
                send_up(HELPER, [c for c in ORDER if c not in EARLY])
        pl.semaphore_wait(reach_sem.at[lm - 1], 1)
        send_down(HELPER)
        remote(dn_hbm.at[pl.ds(share(x), fh), :], wdn.at[dn_rows(HELPER), own], 6, one_sem.at[4], at(MAIN))
        arrived(gi.at[0:2], local_sem.at[1])
        arrived(unit[0 : up_units(HELPER) + NC], send_sem.at[2])
        arrived(unit[0 : 2 * (nx - 1) * len(FORWARDED)], send_sem.at[3])
        arrived(unit[0 : nx * NC], send_sem.at[6])
        arrived(unit[0:4], one_sem.at[6])
        arrived(st2.at[0 : nz * nx], one_sem.at[7])
        finish()

    def main():
        greeted = enter(
            [(MAIN, z, xs[dx], ys[dj]) for dj, dx in pairs] + [at(MAIN, dz) for dz in (1, nz - 1)]
            + [at(HELPER, 0, dx) for dx in range(nx)] + [(HELPER, z, x, yw)]
        )
        pltpu.make_async_copy(res_hbm, raw.at[x, q], local_sem.at[0]).start()
        for src, dst in ((gi_hbm, gi.at[x]), (si_hbm, si.at[x]), (go_hbm, go), (so_hbm, so)):
            pltpu.make_async_copy(src, dst, local_sem.at[1]).start()
        for c in range(NC // 2, NC):
            pltpu.make_async_copy(up_hbm.at[:, up_cols(c, x)], wup.at[c, own, :], local_sem.at[2]).start()
        src = dn_hbm.at[pl.ds(share(x), fh), :]
        pltpu.make_async_copy(src, wdn.at[dn_rows(MAIN), own], local_sem.at[2]).start()
        arrived(unit[0:2], local_sem.at[0])
        arrived(gi, local_sem.at[1])
        st0[0] = of_shard(raw[x, q].astype(F32))
        greeted()

        for dj, dx in pairs:
            remote(st0.at[0], st0.at[dj * nx + dx], 11, one_sem.at[9], (MAIN, z, xs[dx], ys[dj]))
        for dj, dx in pairs:
            remote(raw.at[x, q], raw.at[x, q], 0, one_sem.at[2 + dj], (MAIN, z, xs[dx], ys[dj]))
        for dx in range(1, nx):
            remote(gi.at[x], gi.at[x], 1, one_sem.at[0], at(MAIN, 0, dx))
            remote(si.at[x], si.at[x], 8, one_sem.at[1], at(MAIN, 0, dx))
        send_up(MAIN, ORDER)

        for k in range(lm - 1):
            for dz in (1, nz - 1):
                pl.semaphore_signal(reach_sem.at[k], inc=1, device_id=at(MAIN, dz), device_id_type=MESH)
            pl.semaphore_wait(reach_sem.at[k], 2)

        arrived(st0.at[1 : 2 * nx], one_sem.at[9])
        for dj in range(2):
            st1[z, qs[dj]] = jnp.concatenate(pool(st0[dj * nx : (dj + 1) * nx], width), axis=0)
        for dz in FAR[:-1]:
            remote(st1.at[z], st1.at[z], 9, one_sem.at[8], at(MAIN, dz))
        arrived(gi.at[1:nx], one_sem.at[0])
        arrived(si.at[1:nx], one_sem.at[1])
        for dj in range(2):
            arrived(unit[0 : 2 * (nx - 1 + dj)], one_sem.at[2 + dj])
        arrived(st1.at[1:nz], one_sem.at[8])
        for j in range(2):
            mean, scale = combine(st1[:, j], depth)
            mean, scale = row_to_lanes(mean), row_to_lanes(scale)
            for k in range(nx):
                v = (raw[k, j].astype(F32) - mean) * scale * gi[k] + si[k]
                normed[j * nq : (j + 1) * nq, :, k * width : (k + 1) * width] = v.astype(BF16).reshape(nq, rows, width)

        def partials(blocks, c):
            left = jnp.concatenate([normed[d] for d in blocks], axis=0)
            both = jnp.dot(left, wup[c], preferred_element_type=F32)
            return [both[i * rows : (i + 1) * rows] for i in range(len(blocks))]

        def active(c, s):
            return [di for di in range(2) if s < hops(c, di, nz)]

        def target(c, di, s):
            ahead = hops(c, di, nz) - s
            return zs[ahead] if di == 0 else zs[nz - ahead]

        def pass_on(c, di, s, value):
            rsb[c, s, di] = value.astype(BF16)
            remote(rsb.at[c, s, di], rrb.at[c, s, di], 4, ring_sem.at[c, s], at(MAIN, 1 if di == 0 else nz - 1))

        def spread(c, di, s):
            block = unit[c * nz + (zs[nz - s if s else 0] if di == 0 else zs[s])]
            remote(block, block, 5, ring_sem.at[c, s], at(MAIN, 1 if di == 0 else nz - 1))

        def prepare(c, s):
            blocks = [target(c, di, s) for di in active(c, s)]
            if s == lm - 1:
                blocks.append(z)
            for slot, value in zip(active(c, s) + [2], partials(blocks, c)):
                pbuf[c, slot] = value

        arrived(unit[0 : 2 * NC], local_sem.at[2])
        for c in ORDER:
            arrived(unit[0 : 2 * (nx - 1) + (2 if c < NC // 2 else 0)], up_sem.at[1, c])
            for di, value in zip(active(c, 0), partials([target(c, di, 0) for di in active(c, 0)], c)):
                pass_on(c, di, 0, value)
            prepare(c, 1)
        pl.semaphore_signal(reach_sem.at[lm - 1], inc=1, device_id=at(HELPER), device_id_type=MESH)
        send_down(MAIN)
        for s in range(1, lm + 1):
            for c in ORDER:
                arrived(rrb.at[c, 0, 0 : len(active(c, s - 1))], ring_sem.at[c, s - 1])
                if s < lm:
                    for di in active(c, s):
                        pass_on(c, di, s, pbuf[c, di] + rrb[c, s - 1, di].astype(F32))
                    if s < lm - 1:
                        prepare(c, s + 1)
                else:
                    value = pbuf[c, 2]
                    for di in range(2):
                        value = value + rrb[c, hops(c, di, nz) - 1, di].astype(F32)
                    hid[c * nz + z] = jnp.square(jnp.maximum(value, 0.0)).astype(BF16)
                    for di in range(2):
                        spread(c, di, 0)

        def down(c, ks):
            left = jnp.concatenate([hid[c * nz + zs[k]] for k in ks], axis=0)
            value = jnp.dot(left, wdn[c * cw : (c + 1) * cw, :], preferred_element_type=F32)
            for i, k in enumerate(ks):
                part = value[i * rows : (i + 1) * rows]
                acc[k] = part if c == ORDER[0] else acc[k] + part

        def branch(ks):
            for k in ks:
                o = zs[k]
                sb[o] = acc[k].astype(BF16)
                j, i = lax.div(o, nq), lax.rem(o, nq)
                dj = lax.rem(j + q, 2)
                for dx in (2, 1, 3, 0):
                    cols = pl.ds(pl.multiple_of(xs[dx] * width, width), width)
                    send = functools.partial(
                        remote, sb.at[o, :, cols], rb.at[dj, dx, i], 7, one_sem.at[5], (MAIN, z, xs[dx], y - q + j)
                    )
                    if dx:
                        send()
                    else:
                        pl.when(dj != 0)(send)

        stages = [(0, 1, nz - 1)] + [(k, nz - k) for k in range(2, lm)] + [(lm,)]
        for s in range(1, lm + 1):
            if s == 2:
                arrived(unit[0 : NC * (nx - 1) * 2 + NC], one_sem.at[4])
            for c in ORDER:
                arrived(unit[0 : len(active(c, s - 1))], ring_sem.at[c, s - 1])
                for di in active(c, s):
                    spread(c, di, s)
                if s > 1:
                    down(c, stages[s - 2] if s < lm else stages[s - 1])
            if 1 < s < lm:
                branch(stages[s - 2])
            if s == lm - 1:
                for c in ORDER:
                    down(c, stages[s - 1])
                branch(stages[s - 1])
        branch(stages[lm - 1])

        blocks = pl.ds(pl.multiple_of(q * nq, nq), nq)
        total = 2.0**0.25 * normed[blocks, :, own].astype(F32) + sb[blocks, :, own].astype(F32)
        arrived(unit[0 : 2 * len(pairs)], one_sem.at[5])
        for dj, dx in pairs:
            total = total + rb[dj, dx].astype(F32)
        total = total.reshape(tokens, width)
        st2[0] = of_shard(total)
        tot[...] = total
        for core in (MAIN, HELPER):
            for dz in FAR:
                for dx in (2, 1, 3, 0):
                    k = dz * nx + dx
                    if k or core == HELPER:
                        remote(st2.at[0], st2.at[k], 10, one_sem.at[7], at(core, dz, dx))
            if core == MAIN:
                remote(tot, tot, 0, one_sem.at[6], at(HELPER))
        arrived(st2.at[1 : nz * nx], one_sem.at[7])
        finish()

        for group, ref in (
            (0, unit[0 : 2 * len(pairs) + 4]),
            (1, gi.at[1:nx]),
            (8, si.at[1:nx]),
            (2, unit[0 : up_units(MAIN)]),
            (4, unit[0 : len(pairs) * NC]),
            (5, unit[0 : len(pairs) * NC]),
            (6, unit[0 : (nx - 1) * NC]),
            (7, unit[0 : 2 * len(pairs)]),
            (9, st1.at[1:nz]),
            (10, st2.at[1 : 2 * nz * nx]),
            (11, st0.at[1 : 2 * nx]),
        ):
            arrived(ref, send_sem.at[group])

    pl.when(r == MAIN)(main)
    pl.when(r == HELPER)(helper)


def per_device(nz, nx, residual_in, gain_in, shift_in, up_weight, down_weight, gain_out, shift_out):
    tokens, width = residual_in.shape
    nq, depth = nz // 2, nx * width
    rows = tokens // nq
    fc = up_weight.shape[1] // nx
    cw = fc // NC
    dma = pltpu.SemaphoreType.DMA
    row = (1, width)
    return pl.pallas_call(
        functools.partial(kernel, nz, nx),
        out_shape=pltpu.VMEM((tokens, width), BF16),
        in_specs=[pl.BlockSpec(memory_space=pl.ANY)] * 7,
        out_specs=pl.BlockSpec(memory_space=pltpu.VMEM),
        scratch_shapes=[
            pltpu.VMEM((nx, 2, tokens, width), BF16),
            pltpu.VMEM((nx, *row), F32),
            pltpu.VMEM((nx, *row), F32),
            pltpu.VMEM(row, F32),
            pltpu.VMEM(row, F32),
            pltpu.VMEM((NC, depth, cw), BF16),
            pltpu.VMEM((fc, depth), BF16),
            pltpu.VMEM((2 * nx, 2, tokens), F32),
            pltpu.VMEM((nz, 2, 2, tokens), F32),
            pltpu.VMEM((nz, rows, depth), BF16),
            pltpu.VMEM((NC, 3, rows, cw), F32),
            pltpu.VMEM((NC, nq, 2, rows, cw), BF16),
            pltpu.VMEM((NC, nq, 2, rows, cw), BF16),
            pltpu.VMEM((NC * nz, rows, cw), BF16),
            pltpu.VMEM((nz, rows, depth), F32),
            pltpu.VMEM((nz, rows, depth), BF16),
            pltpu.VMEM((2, nx, nq, rows, width), BF16),
            pltpu.VMEM((2 * nz * nx, 2, tokens), F32),
            pltpu.VMEM((tokens, width), F32),
            dma((3,)),
            dma((12,)),
            dma((2, NC)),
            dma((10,)),
            dma((NC, nq)),
            pltpu.SemaphoreType.REGULAR((nq,)),
        ],
        compiler_params=pltpu.CompilerParams(collective_id=0, has_side_effects=True),
    )(
        residual_in, gain_in.reshape(row), shift_in.reshape(row), up_weight, down_weight,
        gain_out.reshape(row), shift_out.reshape(row),
    )


def solution(mesh):
    nz, nx = 8, 4
    split = Mesh(
        mesh.devices.reshape(mesh.shape["ra"], nz, nx, mesh.shape["dp"]), ("ra", "cb_0", "cb_1", "dp")
    )
    placed = (P("dp", CB), P(CB), P(CB), P(CB, "ra"), P("ra", CB), P(CB), P(CB))
    return jax.shard_map(
        functools.partial(per_device, nz, nx), mesh=split, in_specs=placed, out_specs=P("dp", CB), check_vma=False
    )
```

```python
import functools

import jax
import jax.numpy as jnp
from jax import lax
from jax.experimental import pallas as pl
from jax.experimental.pallas import tpu as pltpu
from jax.sharding import Mesh
from jax.sharding import PartitionSpec as P

CB = ("cb_0", "cb_1")
MESH = pl.DeviceIdType.MESH
NC = 8
ORDER = (0, 5, 1, 3, 6, 2, 7, 4)
FORWARDED = (0, 1, 2, 4)
EARLY = (0, 1, 2)
FAR = (4, 3, 5, 2, 6, 1, 7, 0)
MAIN, HELPER = 1, 0
EPS = 1e-05
F32 = jnp.float32
BF16 = jnp.bfloat16


def hops(c, di, nz):
    return nz // 2 - (ORDER.index(c) + di) % 2


def columns_to_rows(a, b):
    n = a.shape[0]
    lane = lax.broadcasted_iota(jnp.int32, (n, 128), 1)
    both = jnp.where(lane == 0, a, jnp.where(lane == 1, b, 0.0))
    return both.T[0:2, :]


def row_to_lanes(row):
    return jnp.broadcast_to(row, (128, row.shape[1])).T


def pool(stats, count):
    sums, squares = stats[:, 0, :], stats[:, 1, :]
    total = jnp.sum(sums, axis=0, keepdims=True)
    apart = sums / count - total / (stats.shape[0] * count)
    return total, jnp.sum(squares, axis=0, keepdims=True) + count * jnp.sum(apart * apart, axis=0, keepdims=True)


def combine(stats, count):
    total, square = pool(stats, count)
    whole = stats.shape[0] * count
    return total / whole, lax.rsqrt(square / whole + EPS)


def of_shard(values):
    sums = jnp.sum(values, axis=1, keepdims=True)
    apart = values - sums / values.shape[1]
    return columns_to_rows(sums, jnp.sum(apart * apart, axis=1, keepdims=True))


def kernel(
    nz, nx, res_hbm, gi_hbm, si_hbm, up_hbm, dn_hbm, go_hbm, so_hbm, out_ref,
    raw, gi, si, go, so, wup, wdn, st0, st1, normed, pbuf, rsb, rrb, hid, acc, sb, rb, st2, tot,
    local_sem, send_sem, raw_sem, up_sem, one_sem, ring_sem, reach_sem,
):
    tokens, width = res_hbm.shape
    nq = nz // 2
    rows = tokens // nq
    depth = nx * width
    fc = wdn.shape[0]
    fh = fc // 2
    cw = fc // NC
    lm = nz // 2
    hw = width // 2

    r = lax.axis_index("ra")
    z = lax.axis_index("cb_0")
    x = lax.axis_index("cb_1")
    y = lax.axis_index("dp")
    q = lax.rem(y, 2)
    pf = lax.rem(lax.div(y + 1, 2), 2)
    w = lax.div(y, 2)
    yw = 3 - y
    xs = [lax.rem(x + k, nx) for k in range(nx)]
    zs = [lax.rem(z + k, nz) for k in range(nz)]
    ys = [y, y + 1 - 2 * q]
    qs = [q, 1 - q]
    pairs = [(dj, dx) for dx in (2, 1, 3, 0) for dj in (1, 0) if dx or dj]
    own = pl.ds(pl.multiple_of(x * width, width), width)
    unit = hid.at

    def at(core, dz=0, dx=0):
        return (core, zs[dz], xs[dx], y)

    def enter(peers):
        barrier = pltpu.get_barrier_semaphore()
        for peer in peers:
            pl.semaphore_signal(barrier, inc=1, device_id=peer, device_id_type=MESH)
        return lambda: pl.semaphore_wait(barrier, len(peers))

    def remote(src, dst, group, recv, peer):
        copy = pltpu.make_async_remote_copy(
            src_ref=src, dst_ref=dst, send_sem=send_sem.at[group], recv_sem=recv, device_id=peer, device_id_type=MESH
        )
        copy.start()

    def arrived(ref, sem):
        pltpu.make_async_copy(ref, ref, sem).wait()

    def share(xd):
        return pl.multiple_of((xd * 2 + pf) * fh, fh)

    def up_cols(c, xd):
        return pl.ds(pl.multiple_of(share(xd) + c % (NC // 2) * cw, cw), cw)

    def up_rows(xd, part):
        return pl.ds(pl.multiple_of(xd * width + part * hw, hw), hw)

    def dn_rows(core):
        return pl.ds(core * fh, fh)

    def send_up(core, chunks):
        for c in chunks:
            if c // (NC // 2) == core:
                for dx in (2, 1, 3):
                    if c in FORWARDED:
                        part = pl.ds(pl.multiple_of(w * hw, hw), hw)
                        dst = wup.at[c, up_rows(x, w), :]
                        remote(up_hbm.at[part, up_cols(c, xs[dx])], dst, 2, up_sem.at[0, c], at(HELPER, 0, dx))
                    else:
                        dst = wup.at[c, own, :]
                        remote(up_hbm.at[:, up_cols(c, xs[dx])], dst, 2, up_sem.at[1, c], at(MAIN, 0, dx))
                if core == HELPER:
                    remote(up_hbm.at[:, up_cols(c, x)], wup.at[c, own, :], 2, up_sem.at[1, c], at(MAIN))

    def up_units(core):
        return sum((nx - 1) * (1 if c in FORWARDED else 2) for c in ORDER if c // (NC // 2) == core)

    def send_down(core):
        for dx in (2, 1, 3):
            src = dn_hbm.at[pl.ds(share(xs[dx]), fh), :]
            remote(src, wdn.at[dn_rows(core), own], 6, one_sem.at[4], at(MAIN, 0, dx))

    def finish():
        mean, scale = combine(st2[0 : nz * nx], width)
        out = (tot[...] - row_to_lanes(mean)) * row_to_lanes(scale) * go[...] + so[...]
        out_ref[...] = out.astype(BF16)

    def helper():
        greeted = enter([(MAIN, z, x, yw), at(MAIN)] + [at(core, 0, dx) for dx in range(1, nx) for core in (0, 1)])
        pltpu.make_async_copy(go_hbm, go, local_sem.at[1]).start()
        pltpu.make_async_copy(so_hbm, so, local_sem.at[1]).start()
        early = [(c, dx) for c in EARLY for dx in (2, 1, 3)]
        part = pl.ds(pl.multiple_of(w * hw, hw), hw)
        for i, (c, dx) in enumerate(early):
            pltpu.make_async_copy(up_hbm.at[part, up_cols(c, xs[dx])], unit[i], local_sem.at[0]).start()
        arrived(unit[0 : len(early)], local_sem.at[0])
        greeted()
        for i, (c, dx) in enumerate(early):
            remote(unit[i], wup.at[c, up_rows(x, w), :], 2, up_sem.at[0, c], at(HELPER, 0, dx))
        for c in EARLY:
            remote(up_hbm.at[:, up_cols(c, x)], wup.at[c, own, :], 2, up_sem.at[1, c], at(MAIN))
        for c in FORWARDED:
            arrived(unit[0 : nx - 1], up_sem.at[0, c])
            for dx in range(1, nx):
                block = wup.at[c, up_rows(xs[dx], w), :]
                remote(block, block, 3, up_sem.at[1, c], (MAIN, z, x, yw))
            for dx in range(1, nx):
                block = wup.at[c, up_rows(xs[dx], w), :]
                remote(block, block, 3, up_sem.at[1, c], at(MAIN))
            if c == FORWARDED[0]:
                send_up(HELPER, [c for c in ORDER if c not in EARLY])
        pl.semaphore_wait(reach_sem.at[lm - 1], 1)
        send_down(HELPER)
        remote(dn_hbm.at[pl.ds(share(x), fh), :], wdn.at[dn_rows(HELPER), own], 6, one_sem.at[4], at(MAIN))
        arrived(gi.at[0:2], local_sem.at[1])
        arrived(unit[0 : up_units(HELPER) + NC], send_sem.at[2])
        arrived(unit[0 : 2 * (nx - 1) * len(FORWARDED)], send_sem.at[3])
        arrived(unit[0 : nx * NC], send_sem.at[6])
        arrived(unit[0:4], one_sem.at[6])
        arrived(st2.at[0 : nz * nx], one_sem.at[7])
        finish()

    def main():
        greeted = enter(
            [(MAIN, z, xs[dx], ys[dj]) for dj, dx in pairs] + [at(MAIN, dz) for dz in (1, nz - 1)]
            + [at(HELPER, 0, dx) for dx in range(nx)] + [(HELPER, z, x, yw)]
        )
        pltpu.make_async_copy(res_hbm, raw.at[x, q], local_sem.at[0]).start()
        for src, dst in ((gi_hbm, gi.at[x]), (si_hbm, si.at[x]), (go_hbm, go), (so_hbm, so)):
            pltpu.make_async_copy(src, dst, local_sem.at[1]).start()
        for c in range(NC // 2, NC):
            pltpu.make_async_copy(up_hbm.at[:, up_cols(c, x)], wup.at[c, own, :], local_sem.at[2]).start()
        src = dn_hbm.at[pl.ds(share(x), fh), :]
        pltpu.make_async_copy(src, wdn.at[dn_rows(MAIN), own], local_sem.at[2]).start()
        arrived(unit[0:2], local_sem.at[0])
        arrived(gi, local_sem.at[1])
        st0[0] = of_shard(raw[x, q].astype(F32))
        greeted()

        for dj, dx in pairs:
            remote(st0.at[0], st0.at[dj * nx + dx], 11, one_sem.at[9], (MAIN, z, xs[dx], ys[dj]))
        for dx in (2, 1, 3):
            remote(raw.at[x, q], raw.at[x, q], 0, raw_sem.at[dx], at(MAIN, 0, dx))
        mate = (MAIN, z, x, ys[1])
        remote(raw.at[x, q], raw.at[x, q], 0, raw_sem.at[0], mate)
        for dx in range(1, nx):
            remote(gi.at[x], gi.at[x], 1, one_sem.at[0], at(MAIN, 0, dx))
            remote(si.at[x], si.at[x], 8, one_sem.at[1], at(MAIN, 0, dx))
        send_up(MAIN, range(NC))

        for k in range(lm - 1):
            for dz in (1, nz - 1):
                pl.semaphore_signal(reach_sem.at[k], inc=1, device_id=at(MAIN, dz), device_id_type=MESH)
            pl.semaphore_wait(reach_sem.at[k], 2)

        arrived(st0.at[1 : 2 * nx], one_sem.at[9])
        for dj in range(2):
            st1[z, qs[dj]] = jnp.concatenate(pool(st0[dj * nx : (dj + 1) * nx], width), axis=0)
        for dz in FAR[:-1]:
            remote(st1.at[z], st1.at[z], 9, one_sem.at[8], at(MAIN, dz))
        for dx in (1, 3, 2):
            block = raw.at[xs[nx - dx], q]
            arrived(block, raw_sem.at[dx])
            remote(block, block, 0, raw_sem.at[0], mate)
        arrived(gi.at[1:nx], one_sem.at[0])
        arrived(si.at[1:nx], one_sem.at[1])
        arrived(unit[0 : 2 * nx], raw_sem.at[0])
        arrived(st1.at[1:nz], one_sem.at[8])
        for j in range(2):
            mean, scale = combine(st1[:, j], depth)
            mean, scale = row_to_lanes(mean), row_to_lanes(scale)
            for k in range(nx):
                v = (raw[k, j].astype(F32) - mean) * scale * gi[k] + si[k]
                normed[j * nq : (j + 1) * nq, :, k * width : (k + 1) * width] = v.astype(BF16).reshape(nq, rows, width)

        def products(ks, c):
            left = jnp.concatenate([normed[zs[k]] for k in ks], axis=0)
            value = jnp.dot(left, wup[c], preferred_element_type=F32)
            return [value[i * rows : (i + 1) * rows] for i in range(len(ks))]

        def active(c, s):
            return [di for di in range(2) if s < hops(c, di, nz)]

        def target(c, di, s):
            ahead = hops(c, di, nz) - s
            return ahead if di == 0 else nz - ahead

        def pass_on(c, di, s, value):
            rsb[c, s, di] = value.astype(BF16)
            remote(rsb.at[c, s, di], rrb.at[c, s, di], 4, ring_sem.at[c, s], at(MAIN, 1 if di == 0 else nz - 1))

        def spread(c, di, s):
            block = unit[c * nz + (zs[nz - s if s else 0] if di == 0 else zs[s])]
            remote(block, block, 5, ring_sem.at[c, s], at(MAIN, 1 if di == 0 else nz - 1))

        arrived(unit[0 : 2 * NC], local_sem.at[2])
        for c in ORDER:
            arrived(unit[0 : 2 * (nx - 1) + (2 if c < NC // 2 else 0)], up_sem.at[1, c])
            near = [target(c, di, s) for s in range(2) for di in range(2)]
            values = products(near, c)
            for di in range(2):
                pass_on(c, di, 0, values[di])
                pbuf[c, near[2 + di]] = values[2 + di]
        pl.semaphore_signal(reach_sem.at[lm - 1], inc=1, device_id=at(HELPER), device_id_type=MESH)
        send_down(MAIN)
        for s in range(1, lm + 1):
            for c in ORDER:
                arrived(rrb.at[c, 0, 0 : len(active(c, s - 1))], ring_sem.at[c, s - 1])
                if s < lm:
                    for di in active(c, s):
                        pass_on(c, di, s, pbuf[c, target(c, di, s)] + rrb[c, s - 1, di].astype(F32))
                    if s == 1:
                        far = [target(c, di, t) for t in range(2, lm) for di in active(c, t)] + [0]
                        for k, value in zip(far, products(far, c)):
                            pbuf[c, k] = value
                else:
                    value = pbuf[c, 0]
                    for di in range(2):
                        value = value + rrb[c, hops(c, di, nz) - 1, di].astype(F32)
                    hid[c * nz + z] = jnp.square(jnp.maximum(value, 0.0)).astype(BF16)
                    for di in range(2):
                        spread(c, di, 0)

        def down(c, ks):
            place = ORDER.index(c)
            if place % 2 == 0:
                return
            pair = (ORDER[place - 1], c)
            halves = [jnp.concatenate([hid[half * nz + zs[k]] for k in ks], axis=0) for half in pair]
            right = jnp.concatenate([wdn[half * cw : (half + 1) * cw, :] for half in pair], axis=0)
            value = jnp.dot(jnp.concatenate(halves, axis=1), right, preferred_element_type=F32)
            for i, k in enumerate(ks):
                part = value[i * rows : (i + 1) * rows]
                acc[k] = part if place == 1 else acc[k] + part

        def branch(ks):
            for k in ks:
                o = zs[k]
                sb[o] = acc[k].astype(BF16)
                j, i = lax.div(o, nq), lax.rem(o, nq)
                dj = lax.rem(j + q, 2)
                for dx in (2, 1, 3, 0):
                    cols = pl.ds(pl.multiple_of(xs[dx] * width, width), width)
                    send = functools.partial(
                        remote, sb.at[o, :, cols], rb.at[dj, dx, i], 7, one_sem.at[5], (MAIN, z, xs[dx], y - q + j)
                    )
                    if dx:
                        send()
                    else:
                        pl.when(dj != 0)(send)

        stages = [(0, 1, nz - 1)] + [(k, nz - k) for k in range(2, lm)] + [(lm,)]
        for s in range(1, lm + 1):
            if s == 2:
                arrived(unit[0 : NC * (nx - 1) * 2 + NC], one_sem.at[4])
            for c in ORDER:
                arrived(unit[0 : len(active(c, s - 1))], ring_sem.at[c, s - 1])
                for di in active(c, s):
                    spread(c, di, s)
                if s > 1:
                    down(c, stages[s - 2] if s < lm else stages[s - 1])
            if 1 < s < lm:
                branch(stages[s - 2])
            if s == lm - 1:
                for c in ORDER:
                    down(c, stages[s - 1])
                branch(stages[s - 1])
        branch(stages[lm - 1])

        blocks = pl.ds(pl.multiple_of(q * nq, nq), nq)
        total = 2.0**0.25 * normed[blocks, :, own].astype(F32) + sb[blocks, :, own].astype(F32)
        arrived(unit[0 : 2 * len(pairs)], one_sem.at[5])
        for dj, dx in pairs:
            total = total + rb[dj, dx].astype(F32)
        total = total.reshape(tokens, width)
        st2[0] = of_shard(total)
        tot[...] = total
        for core in (MAIN, HELPER):
            for dz in FAR:
                for dx in (2, 1, 3, 0):
                    k = dz * nx + dx
                    if k or core == HELPER:
                        remote(st2.at[0], st2.at[k], 10, one_sem.at[7], at(core, dz, dx))
            if core == MAIN:
                remote(tot, tot, 0, one_sem.at[6], at(HELPER))
        arrived(st2.at[1 : nz * nx], one_sem.at[7])
        finish()

        for group, ref in (
            (0, unit[0 : 2 * len(pairs) + 4]),
            (1, gi.at[1:nx]),
            (8, si.at[1:nx]),
            (2, unit[0 : up_units(MAIN)]),
            (4, unit[0 : len(pairs) * NC]),
            (5, unit[0 : len(pairs) * NC]),
            (6, unit[0 : (nx - 1) * NC]),
            (7, unit[0 : 2 * len(pairs)]),
            (9, st1.at[1:nz]),
            (10, st2.at[1 : 2 * nz * nx]),
            (11, st0.at[1 : 2 * nx]),
        ):
            arrived(ref, send_sem.at[group])

    pl.when(r == MAIN)(main)
    pl.when(r == HELPER)(helper)


def per_device(nz, nx, residual_in, gain_in, shift_in, up_weight, down_weight, gain_out, shift_out):
    tokens, width = residual_in.shape
    nq, depth = nz // 2, nx * width
    rows = tokens // nq
    fc = up_weight.shape[1] // nx
    cw = fc // NC
    dma = pltpu.SemaphoreType.DMA
    row = (1, width)
    return pl.pallas_call(
        functools.partial(kernel, nz, nx),
        out_shape=pltpu.VMEM((tokens, width), BF16),
        in_specs=[pl.BlockSpec(memory_space=pl.ANY)] * 7,
        out_specs=pl.BlockSpec(memory_space=pltpu.VMEM),
        scratch_shapes=[
            pltpu.VMEM((nx, 2, tokens, width), BF16),
            pltpu.VMEM((nx, *row), F32),
            pltpu.VMEM((nx, *row), F32),
            pltpu.VMEM(row, F32),
            pltpu.VMEM(row, F32),
            pltpu.VMEM((NC, depth, cw), BF16),
            pltpu.VMEM((fc, depth), BF16),
            pltpu.VMEM((2 * nx, 2, tokens), F32),
            pltpu.VMEM((nz, 2, 2, tokens), F32),
            pltpu.VMEM((nz, rows, depth), BF16),
            pltpu.VMEM((NC, nz, rows, cw), F32),
            pltpu.VMEM((NC, nq, 2, rows, cw), BF16),
            pltpu.VMEM((NC, nq, 2, rows, cw), BF16),
            pltpu.VMEM((NC * nz, rows, cw), BF16),
            pltpu.VMEM((nz, rows, depth), F32),
            pltpu.VMEM((nz, rows, depth), BF16),
            pltpu.VMEM((2, nx, nq, rows, width), BF16),
            pltpu.VMEM((2 * nz * nx, 2, tokens), F32),
            pltpu.VMEM((tokens, width), F32),
            dma((3,)),
            dma((12,)),
            dma((nx,)),
            dma((2, NC)),
            dma((10,)),
            dma((NC, nq)),
            pltpu.SemaphoreType.REGULAR((nq,)),
        ],
        compiler_params=pltpu.CompilerParams(collective_id=0, has_side_effects=True),
    )(
        residual_in, gain_in.reshape(row), shift_in.reshape(row), up_weight, down_weight,
        gain_out.reshape(row), shift_out.reshape(row),
    )


def solution(mesh):
    nz, nx = 8, 4
    split = Mesh(
        mesh.devices.reshape(mesh.shape["ra"], nz, nx, mesh.shape["dp"]), ("ra", "cb_0", "cb_1", "dp")
    )
    placed = (P("dp", CB), P(CB), P(CB), P(CB, "ra"), P("ra", CB), P(CB), P(CB))
    return jax.shard_map(
        functools.partial(per_device, nz, nx), mesh=split, in_specs=placed, out_specs=P("dp", CB), check_vma=False
    )
```

```python
import functools

import jax
import jax.numpy as jnp
from jax import lax
from jax.experimental import pallas as pl
from jax.experimental.pallas import tpu as pltpu
from jax.sharding import Mesh
from jax.sharding import PartitionSpec as P

CB = ("cb_0", "cb_1")
MESH = pl.DeviceIdType.MESH
NC = 8
ORDER = (0, 5, 1, 6, 4, 3, 2, 7)
FORWARDED = (0, 1, 4, 2)
EARLY = (0, 1, 2)
FAR = (4, 3, 5, 2, 6, 1, 7, 0)
MAIN, HELPER = 1, 0
EPS = 1e-05
F32 = jnp.float32
BF16 = jnp.bfloat16


def hops(c, di, nz):
    return nz // 2 - (ORDER.index(c) + di) % 2


def columns_to_rows(a, b):
    n = a.shape[0]
    lane = lax.broadcasted_iota(jnp.int32, (n, 128), 1)
    both = jnp.where(lane == 0, a, jnp.where(lane == 1, b, 0.0))
    return both.T[0:2, :]


def row_to_lanes(row):
    return jnp.broadcast_to(row, (128, row.shape[1])).T


def pool(stats, count):
    sums, squares = stats[:, 0, :], stats[:, 1, :]
    total = jnp.sum(sums, axis=0, keepdims=True)
    apart = sums / count - total / (stats.shape[0] * count)
    return total, jnp.sum(squares, axis=0, keepdims=True) + count * jnp.sum(apart * apart, axis=0, keepdims=True)


def combine(stats, count):
    total, square = pool(stats, count)
    whole = stats.shape[0] * count
    return total / whole, lax.rsqrt(square / whole + EPS)


def of_shard(values):
    sums = jnp.sum(values, axis=1, keepdims=True)
    apart = values - sums / values.shape[1]
    return columns_to_rows(sums, jnp.sum(apart * apart, axis=1, keepdims=True))


def kernel(
    nz, nx, res_hbm, gi_hbm, si_hbm, up_hbm, dn_hbm, go_hbm, so_hbm, out_ref,
    raw, gi, si, go, so, wup, wdn, st0, st1, normed, pbuf, rsb, rrb, hid, acc, sb, rb, st2, tot,
    local_sem, send_sem, raw_sem, up_sem, one_sem, ring_sem, reach_sem,
):
    tokens, width = res_hbm.shape
    nq = nz // 2
    rows = tokens // nq
    depth = nx * width
    fc = wdn.shape[0]
    fh = fc // 2
    cw = fc // NC
    lm = nz // 2
    hw = width // 2

    r = lax.axis_index("ra")
    z = lax.axis_index("cb_0")
    x = lax.axis_index("cb_1")
    y = lax.axis_index("dp")
    q = lax.rem(y, 2)
    pf = lax.rem(lax.div(y + 1, 2), 2)
    w = lax.div(y, 2)
    yw = 3 - y
    xs = [lax.rem(x + k, nx) for k in range(nx)]
    zs = [lax.rem(z + k, nz) for k in range(nz)]
    ys = [y, y + 1 - 2 * q]
    qs = [q, 1 - q]
    pairs = [(dj, dx) for dx in (2, 1, 3, 0) for dj in (1, 0) if dx or dj]
    own = pl.ds(pl.multiple_of(x * width, width), width)
    unit = hid.at

    def at(core, dz=0, dx=0):
        return (core, zs[dz], xs[dx], y)

    def enter(peers):
        barrier = pltpu.get_barrier_semaphore()
        for peer in peers:
            pl.semaphore_signal(barrier, inc=1, device_id=peer, device_id_type=MESH)
        return lambda: pl.semaphore_wait(barrier, len(peers))

    def remote(src, dst, group, recv, peer):
        copy = pltpu.make_async_remote_copy(
            src_ref=src, dst_ref=dst, send_sem=send_sem.at[group], recv_sem=recv, device_id=peer, device_id_type=MESH
        )
        copy.start()

    def arrived(ref, sem):
        pltpu.make_async_copy(ref, ref, sem).wait()

    def share(xd):
        return pl.multiple_of((xd * 2 + pf) * fh, fh)

    def up_cols(c, xd):
        return pl.ds(pl.multiple_of(share(xd) + c % (NC // 2) * cw, cw), cw)

    def up_rows(xd, part):
        return pl.ds(pl.multiple_of(xd * width + part * hw, hw), hw)

    def dn_rows(core):
        return pl.ds(core * fh, fh)

    def send_up(core, chunks):
        for c in chunks:
            if c // (NC // 2) == core:
                for dx in (2, 1, 3):
                    if c in FORWARDED:
                        part = pl.ds(pl.multiple_of(w * hw, hw), hw)
                        dst = wup.at[c, up_rows(x, w), :]
                        remote(up_hbm.at[part, up_cols(c, xs[dx])], dst, 2, up_sem.at[0, c], at(HELPER, 0, dx))
                    else:
                        dst = wup.at[c, own, :]
                        remote(up_hbm.at[:, up_cols(c, xs[dx])], dst, 2, up_sem.at[1, c], at(MAIN, 0, dx))
                if core == HELPER:
                    remote(up_hbm.at[:, up_cols(c, x)], wup.at[c, own, :], 2, up_sem.at[1, c], at(MAIN))

    def up_units(core):
        return sum((nx - 1) * (1 if c in FORWARDED else 2) for c in ORDER if c // (NC // 2) == core)

    def send_down(core):
        for dx in (2, 1, 3):
            src = dn_hbm.at[pl.ds(share(xs[dx]), fh), :]
            remote(src, wdn.at[dn_rows(core), own], 6, one_sem.at[4], at(MAIN, 0, dx))

    def finish():
        mean, scale = combine(st2[0 : nz * nx], width)
        out = (tot[...] - row_to_lanes(mean)) * row_to_lanes(scale) * go[...] + so[...]
        out_ref[...] = out.astype(BF16)

    def helper():
        greeted = enter([(MAIN, z, x, yw), at(MAIN)] + [at(core, 0, dx) for dx in range(1, nx) for core in (0, 1)])
        pltpu.make_async_copy(go_hbm, go, local_sem.at[1]).start()
        pltpu.make_async_copy(so_hbm, so, local_sem.at[1]).start()
        early = [(c, dx) for c in EARLY for dx in (2, 1, 3)]
        part = pl.ds(pl.multiple_of(w * hw, hw), hw)
        for i, (c, dx) in enumerate(early):
            pltpu.make_async_copy(up_hbm.at[part, up_cols(c, xs[dx])], unit[i], local_sem.at[0]).start()
        arrived(unit[0 : len(early)], local_sem.at[0])
        greeted()
        for i, (c, dx) in enumerate(early):
            remote(unit[i], wup.at[c, up_rows(x, w), :], 2, up_sem.at[0, c], at(HELPER, 0, dx))
        for c in EARLY:
            remote(up_hbm.at[:, up_cols(c, x)], wup.at[c, own, :], 2, up_sem.at[1, c], at(MAIN))
        for c in FORWARDED:
            arrived(unit[0 : nx - 1], up_sem.at[0, c])
            for dx in range(1, nx):
                block = wup.at[c, up_rows(xs[dx], w), :]
                remote(block, block, 3, up_sem.at[1, c], (MAIN, z, x, yw))
            for dx in range(1, nx):
                block = wup.at[c, up_rows(xs[dx], w), :]
                remote(block, block, 3, up_sem.at[1, c], at(MAIN))
            if c == FORWARDED[0]:
                send_up(HELPER, [c for c in ORDER if c not in EARLY])
        pl.semaphore_wait(reach_sem.at[lm - 1], 1)
        send_down(HELPER)
        remote(dn_hbm.at[pl.ds(share(x), fh), :], wdn.at[dn_rows(HELPER), own], 6, one_sem.at[4], at(MAIN))
        arrived(gi.at[0:2], local_sem.at[1])
        arrived(unit[0 : up_units(HELPER) + NC], send_sem.at[2])
        arrived(unit[0 : 2 * (nx - 1) * len(FORWARDED)], send_sem.at[3])
        arrived(unit[0 : nx * NC], send_sem.at[6])
        arrived(unit[0:4], one_sem.at[6])
        arrived(st2.at[0 : nz * nx], one_sem.at[7])
        finish()

    def main():
        greeted = enter(
            [(MAIN, z, xs[dx], ys[dj]) for dj, dx in pairs] + [at(MAIN, dz) for dz in (1, nz - 1)]
            + [at(HELPER, 0, dx) for dx in range(nx)] + [(HELPER, z, x, yw)]
        )
        pltpu.make_async_copy(res_hbm, raw.at[x, q], local_sem.at[0]).start()
        for src, dst in ((gi_hbm, gi.at[x]), (si_hbm, si.at[x]), (go_hbm, go), (so_hbm, so)):
            pltpu.make_async_copy(src, dst, local_sem.at[1]).start()
        for c in range(NC // 2, NC):
            pltpu.make_async_copy(up_hbm.at[:, up_cols(c, x)], wup.at[c, own, :], local_sem.at[2]).start()
        src = dn_hbm.at[pl.ds(share(x), fh), :]
        pltpu.make_async_copy(src, wdn.at[dn_rows(MAIN), own], local_sem.at[2]).start()
        arrived(unit[0:2], local_sem.at[0])
        arrived(gi, local_sem.at[1])
        st0[0] = of_shard(raw[x, q].astype(F32))
        greeted()

        for dj, dx in pairs:
            remote(st0.at[0], st0.at[dj * nx + dx], 11, one_sem.at[9], (MAIN, z, xs[dx], ys[dj]))
        halves = [slice(part * tokens // 2, (part + 1) * tokens // 2) for part in range(2)]
        for part, place in enumerate(halves):
            for dx in (2, 1, 3):
                block = raw.at[x, q, place, :]
                remote(block, block, 0, raw_sem.at[2 * dx + part], at(MAIN, 0, dx))
        mate = (MAIN, z, x, ys[1])
        remote(raw.at[x, q], raw.at[x, q], 0, raw_sem.at[0], mate)
        for dx in range(1, nx):
            remote(gi.at[x], gi.at[x], 1, one_sem.at[0], at(MAIN, 0, dx))
            remote(si.at[x], si.at[x], 8, one_sem.at[1], at(MAIN, 0, dx))
        send_up(MAIN, range(NC))

        for k in range(lm - 1):
            for dz in (1, nz - 1):
                pl.semaphore_signal(reach_sem.at[k], inc=1, device_id=at(MAIN, dz), device_id_type=MESH)
            pl.semaphore_wait(reach_sem.at[k], 2)

        arrived(st0.at[1 : 2 * nx], one_sem.at[9])
        for dj in range(2):
            st1[z, qs[dj]] = jnp.concatenate(pool(st0[dj * nx : (dj + 1) * nx], width), axis=0)
        for dz in FAR[:-1]:
            remote(st1.at[z], st1.at[z], 9, one_sem.at[8], at(MAIN, dz))
        for part, place in enumerate(halves):
            for dx in (1, 3, 2):
                block = raw.at[xs[nx - dx], q, place, :]
                arrived(block, raw_sem.at[2 * dx + part])
                remote(block, block, 0, raw_sem.at[0], mate)
        arrived(gi.at[1:nx], one_sem.at[0])
        arrived(si.at[1:nx], one_sem.at[1])
        arrived(unit[0 : 2 * nx], raw_sem.at[0])
        arrived(st1.at[1:nz], one_sem.at[8])
        for j in range(2):
            mean, scale = combine(st1[:, j], depth)
            mean, scale = row_to_lanes(mean), row_to_lanes(scale)
            for k in range(nx):
                v = (raw[k, j].astype(F32) - mean) * scale * gi[k] + si[k]
                normed[j * nq : (j + 1) * nq, :, k * width : (k + 1) * width] = v.astype(BF16).reshape(nq, rows, width)

        def products(ks, c):
            left = jnp.concatenate([normed[zs[k]] for k in ks], axis=0)
            value = jnp.dot(left, wup[c], preferred_element_type=F32)
            return [value[i * rows : (i + 1) * rows] for i in range(len(ks))]

        def active(c, s):
            return [di for di in range(2) if s < hops(c, di, nz)]

        def target(c, di, s):
            ahead = hops(c, di, nz) - s
            return ahead if di == 0 else nz - ahead

        def pass_on(c, di, s, value):
            rsb[c, s, di] = value.astype(BF16)
            remote(rsb.at[c, s, di], rrb.at[c, s, di], 4, ring_sem.at[c, s], at(MAIN, 1 if di == 0 else nz - 1))

        def spread(c, di, s):
            block = unit[c * nz + (zs[nz - s if s else 0] if di == 0 else zs[s])]
            remote(block, block, 5, ring_sem.at[c, s], at(MAIN, 1 if di == 0 else nz - 1))

        arrived(unit[0 : 2 * NC], local_sem.at[2])
        for c in ORDER:
            arrived(unit[0 : 2 * (nx - 1) + (2 if c < NC // 2 else 0)], up_sem.at[1, c])
            near = [target(c, di, s) for s in range(2) for di in range(2)]
            values = products(near, c)
            for di in range(2):
                pass_on(c, di, 0, values[di])
                pbuf[c, near[2 + di]] = values[2 + di]
        pl.semaphore_signal(reach_sem.at[lm - 1], inc=1, device_id=at(HELPER), device_id_type=MESH)
        send_down(MAIN)
        for s in range(1, lm + 1):
            for c in ORDER:
                arrived(rrb.at[c, 0, 0 : len(active(c, s - 1))], ring_sem.at[c, s - 1])
                if s < lm:
                    for di in active(c, s):
                        pass_on(c, di, s, pbuf[c, target(c, di, s)] + rrb[c, s - 1, di].astype(F32))
                    if s == 1:
                        far = [target(c, di, t) for t in range(2, lm) for di in active(c, t)] + [0]
                        for k, value in zip(far, products(far, c)):
                            pbuf[c, k] = value
                else:
                    value = pbuf[c, 0]
                    for di in range(2):
                        value = value + rrb[c, hops(c, di, nz) - 1, di].astype(F32)
                    hid[c * nz + z] = jnp.square(jnp.maximum(value, 0.0)).astype(BF16)
                    for di in range(2):
                        spread(c, di, 0)

        def down(c, ks):
            place = ORDER.index(c)
            if place % 2 == 0:
                return
            pair = (ORDER[place - 1], c)
            halves = [jnp.concatenate([hid[half * nz + zs[k]] for k in ks], axis=0) for half in pair]
            right = jnp.concatenate([wdn[half * cw : (half + 1) * cw, :] for half in pair], axis=0)
            value = jnp.dot(jnp.concatenate(halves, axis=1), right, preferred_element_type=F32)
            for i, k in enumerate(ks):
                part = value[i * rows : (i + 1) * rows]
                acc[k] = part if place == 1 else acc[k] + part

        def branch(ks):
            for k in ks:
                o = zs[k]
                sb[o] = acc[k].astype(BF16)
                j, i = lax.div(o, nq), lax.rem(o, nq)
                dj = lax.rem(j + q, 2)
                for dx in (2, 1, 3, 0):
                    cols = pl.ds(pl.multiple_of(xs[dx] * width, width), width)
                    send = functools.partial(
                        remote, sb.at[o, :, cols], rb.at[dj, dx, i], 7, one_sem.at[5], (MAIN, z, xs[dx], y - q + j)
                    )
                    if dx:
                        send()
                    else:
                        pl.when(dj != 0)(send)

        stages = [(0, 1, nz - 1)] + [(k, nz - k) for k in range(2, lm)] + [(lm,)]
        for s in range(1, lm + 1):
            if s == 2:
                arrived(unit[0 : NC * (nx - 1) * 2 + NC], one_sem.at[4])
            for c in ORDER:
                arrived(unit[0 : len(active(c, s - 1))], ring_sem.at[c, s - 1])
                for di in active(c, s):
                    spread(c, di, s)
                if s > 1:
                    down(c, stages[s - 2] if s < lm else stages[s - 1])
            if 1 < s < lm:
                branch(stages[s - 2])
            if s == lm - 1:
                for c in ORDER:
                    down(c, stages[s - 1])
                branch(stages[s - 1])
        branch(stages[lm - 1])

        blocks = pl.ds(pl.multiple_of(q * nq, nq), nq)
        total = 2.0**0.25 * normed[blocks, :, own].astype(F32) + sb[blocks, :, own].astype(F32)
        arrived(unit[0 : 2 * len(pairs)], one_sem.at[5])
        for dj, dx in pairs:
            total = total + rb[dj, dx].astype(F32)
        total = total.reshape(tokens, width)
        st2[0] = of_shard(total)
        tot[...] = total
        for core in (MAIN, HELPER):
            for dz in FAR:
                for dx in (2, 1, 3, 0):
                    k = dz * nx + dx
                    if k or core == HELPER:
                        remote(st2.at[0], st2.at[k], 10, one_sem.at[7], at(core, dz, dx))
            if core == MAIN:
                remote(tot, tot, 0, one_sem.at[6], at(HELPER))
        arrived(st2.at[1 : nz * nx], one_sem.at[7])
        finish()

        for group, ref in (
            (0, unit[0 : 2 * len(pairs) + 4]),
            (1, gi.at[1:nx]),
            (8, si.at[1:nx]),
            (2, unit[0 : up_units(MAIN)]),
            (4, unit[0 : len(pairs) * NC]),
            (5, unit[0 : len(pairs) * NC]),
            (6, unit[0 : (nx - 1) * NC]),
            (7, unit[0 : 2 * len(pairs)]),
            (9, st1.at[1:nz]),
            (10, st2.at[1 : 2 * nz * nx]),
            (11, st0.at[1 : 2 * nx]),
        ):
            arrived(ref, send_sem.at[group])

    pl.when(r == MAIN)(main)
    pl.when(r == HELPER)(helper)


def per_device(nz, nx, residual_in, gain_in, shift_in, up_weight, down_weight, gain_out, shift_out):
    tokens, width = residual_in.shape
    nq, depth = nz // 2, nx * width
    rows = tokens // nq
    fc = up_weight.shape[1] // nx
    cw = fc // NC
    dma = pltpu.SemaphoreType.DMA
    row = (1, width)
    return pl.pallas_call(
        functools.partial(kernel, nz, nx),
        out_shape=pltpu.VMEM((tokens, width), BF16),
        in_specs=[pl.BlockSpec(memory_space=pl.ANY)] * 7,
        out_specs=pl.BlockSpec(memory_space=pltpu.VMEM),
        scratch_shapes=[
            pltpu.VMEM((nx, 2, tokens, width), BF16),
            pltpu.VMEM((nx, *row), F32),
            pltpu.VMEM((nx, *row), F32),
            pltpu.VMEM(row, F32),
            pltpu.VMEM(row, F32),
            pltpu.VMEM((NC, depth, cw), BF16),
            pltpu.VMEM((fc, depth), BF16),
            pltpu.VMEM((2 * nx, 2, tokens), F32),
            pltpu.VMEM((nz, 2, 2, tokens), F32),
            pltpu.VMEM((nz, rows, depth), BF16),
            pltpu.VMEM((NC, nz, rows, cw), F32),
            pltpu.VMEM((NC, nq, 2, rows, cw), BF16),
            pltpu.VMEM((NC, nq, 2, rows, cw), BF16),
            pltpu.VMEM((NC * nz, rows, cw), BF16),
            pltpu.VMEM((nz, rows, depth), F32),
            pltpu.VMEM((nz, rows, depth), BF16),
            pltpu.VMEM((2, nx, nq, rows, width), BF16),
            pltpu.VMEM((2 * nz * nx, 2, tokens), F32),
            pltpu.VMEM((tokens, width), F32),
            dma((3,)),
            dma((12,)),
            dma((2 * nx,)),
            dma((2, NC)),
            dma((10,)),
            dma((NC, nq)),
            pltpu.SemaphoreType.REGULAR((nq,)),
        ],
        compiler_params=pltpu.CompilerParams(collective_id=0, has_side_effects=True),
    )(
        residual_in, gain_in.reshape(row), shift_in.reshape(row), up_weight, down_weight,
        gain_out.reshape(row), shift_out.reshape(row),
    )


def solution(mesh):
    nz, nx = 8, 4
    split = Mesh(
        mesh.devices.reshape(mesh.shape["ra"], nz, nx, mesh.shape["dp"]), ("ra", "cb_0", "cb_1", "dp")
    )
    placed = (P("dp", CB), P(CB), P(CB), P(CB, "ra"), P("ra", CB), P(CB), P(CB))
    return jax.shard_map(
        functools.partial(per_device, nz, nx), mesh=split, in_specs=placed, out_specs=P("dp", CB), check_vma=False
    )
```

```python
import functools

import jax
import jax.numpy as jnp
from jax import lax
from jax.experimental import pallas as pl
from jax.experimental.pallas import tpu as pltpu
from jax.sharding import Mesh
from jax.sharding import PartitionSpec as P

CB = ("cb_0", "cb_1")
MESH = pl.DeviceIdType.MESH
NC = 8
ORDER = (0, 5, 1, 6, 4, 3, 2, 7)
FORWARDED = (0, 1, 4, 2)
EARLY = (0, 1, 2)
FAR = (4, 3, 5, 2, 6, 1, 7, 0)
MAIN, HELPER = 1, 0
EPS = 1e-05
F32 = jnp.float32
BF16 = jnp.bfloat16


def hops(c, di, nz):
    return nz // 2 - (ORDER.index(c) + di) % 2


def columns_to_rows(a, b):
    n = a.shape[0]
    lane = lax.broadcasted_iota(jnp.int32, (n, 128), 1)
    both = jnp.where(lane == 0, a, jnp.where(lane == 1, b, 0.0))
    return both.T[0:2, :]


def row_to_lanes(row):
    return jnp.broadcast_to(row, (128, row.shape[1])).T


def pool(stats, count):
    sums, squares = stats[:, 0, :], stats[:, 1, :]
    total = jnp.sum(sums, axis=0, keepdims=True)
    apart = sums / count - total / (stats.shape[0] * count)
    return total, jnp.sum(squares, axis=0, keepdims=True) + count * jnp.sum(apart * apart, axis=0, keepdims=True)


def combine(stats, count):
    total, square = pool(stats, count)
    whole = stats.shape[0] * count
    return total / whole, lax.rsqrt(square / whole + EPS)


def of_shard(values):
    sums = jnp.sum(values, axis=1, keepdims=True)
    apart = values - sums / values.shape[1]
    return columns_to_rows(sums, jnp.sum(apart * apart, axis=1, keepdims=True))


def kernel(
    nz, nx, res_hbm, gi_hbm, si_hbm, up_hbm, dn_hbm, go_hbm, so_hbm, out_ref,
    raw, gi, si, go, so, wup, wdn, st0, st1, normed, pbuf, rsb, rrb, hid, acc, sb, rb, st2, tot,
    local_sem, send_sem, raw_sem, up_sem, one_sem, ring_sem, reach_sem,
):
    tokens, width = res_hbm.shape
    nq = nz // 2
    rows = tokens // nq
    depth = nx * width
    fc = wdn.shape[0]
    fh = fc // 2
    cw = fc // NC
    lm = nz // 2
    hw = width // 2

    r = lax.axis_index("ra")
    z = lax.axis_index("cb_0")
    x = lax.axis_index("cb_1")
    y = lax.axis_index("dp")
    q = lax.rem(y, 2)
    pf = lax.rem(lax.div(y + 1, 2), 2)
    w = lax.div(y, 2)
    yw = 3 - y
    xs = [lax.rem(x + k, nx) for k in range(nx)]
    zs = [lax.rem(z + k, nz) for k in range(nz)]
    ys = [y, y + 1 - 2 * q]
    qs = [q, 1 - q]
    pairs = [(dj, dx) for dx in (2, 1, 3, 0) for dj in (1, 0) if dx or dj]
    own = pl.ds(pl.multiple_of(x * width, width), width)
    unit = hid.at

    def at(core, dz=0, dx=0):
        return (core, zs[dz], xs[dx], y)

    def enter(peers):
        barrier = pltpu.get_barrier_semaphore()
        for peer in peers:
            pl.semaphore_signal(barrier, inc=1, device_id=peer, device_id_type=MESH)
        return lambda: pl.semaphore_wait(barrier, len(peers))

    def remote(src, dst, group, recv, peer):
        copy = pltpu.make_async_remote_copy(
            src_ref=src, dst_ref=dst, send_sem=send_sem.at[group], recv_sem=recv, device_id=peer, device_id_type=MESH
        )
        copy.start()

    def arrived(ref, sem):
        pltpu.make_async_copy(ref, ref, sem).wait()

    def share(xd):
        return pl.multiple_of((xd * 2 + pf) * fh, fh)

    def up_cols(c, xd):
        return pl.ds(pl.multiple_of(share(xd) + c % (NC // 2) * cw, cw), cw)

    def up_rows(xd, part):
        return pl.ds(pl.multiple_of(xd * width + part * hw, hw), hw)

    def dn_rows(core):
        return pl.ds(core * fh, fh)

    def send_up(core, chunks):
        for c in chunks:
            if c // (NC // 2) == core:
                for dx in (2, 1, 3):
                    if c in FORWARDED:
                        part = pl.ds(pl.multiple_of(w * hw, hw), hw)
                        dst = wup.at[c, up_rows(x, w), :]
                        remote(up_hbm.at[part, up_cols(c, xs[dx])], dst, 2, up_sem.at[NC + FORWARDED.index(c)], at(HELPER, 0, dx))
                    else:
                        dst = wup.at[c, own, :]
                        remote(up_hbm.at[:, up_cols(c, xs[dx])], dst, 2, up_sem.at[c], at(MAIN, 0, dx))
                if core == HELPER:
                    remote(up_hbm.at[:, up_cols(c, x)], wup.at[c, own, :], 2, up_sem.at[c], at(MAIN))

    def up_units(core):
        return sum((nx - 1) * (1 if c in FORWARDED else 2) for c in ORDER if c // (NC // 2) == core)

    def send_down(core):
        for dx in (2, 1, 3):
            src = dn_hbm.at[pl.ds(share(xs[dx]), fh), :]
            remote(src, wdn.at[dn_rows(core), own], 6, one_sem.at[4], at(MAIN, 0, dx))

    def finish():
        mean, scale = combine(st2[0 : nz * nx], width)
        out = (tot[...] - row_to_lanes(mean)) * row_to_lanes(scale) * go[...] + so[...]
        out_ref[...] = out.astype(BF16)

    def helper():
        greeted = enter([(MAIN, z, x, yw), at(MAIN)] + [at(core, 0, dx) for dx in range(1, nx) for core in (0, 1)])
        pltpu.make_async_copy(go_hbm, go, local_sem.at[1]).start()
        pltpu.make_async_copy(so_hbm, so, local_sem.at[1]).start()
        early = [(c, dx) for c in EARLY for dx in (2, 1, 3)]
        part = pl.ds(pl.multiple_of(w * hw, hw), hw)
        for i, (c, dx) in enumerate(early):
            pltpu.make_async_copy(up_hbm.at[part, up_cols(c, xs[dx])], unit[i], local_sem.at[0]).start()
        arrived(unit[0 : len(early)], local_sem.at[0])
        greeted()
        for i, (c, dx) in enumerate(early):
            remote(unit[i], wup.at[c, up_rows(x, w), :], 2, up_sem.at[NC + FORWARDED.index(c)], at(HELPER, 0, dx))
        for c in EARLY:
            remote(up_hbm.at[:, up_cols(c, x)], wup.at[c, own, :], 2, up_sem.at[c], at(MAIN))
        for c in FORWARDED:
            arrived(unit[0 : nx - 1], up_sem.at[NC + FORWARDED.index(c)])
            for dx in range(1, nx):
                block = wup.at[c, up_rows(xs[dx], w), :]
                remote(block, block, 3, up_sem.at[c], (MAIN, z, x, yw))
            for dx in range(1, nx):
                block = wup.at[c, up_rows(xs[dx], w), :]
                remote(block, block, 3, up_sem.at[c], at(MAIN))
            if c == FORWARDED[0]:
                send_up(HELPER, [c for c in ORDER if c not in EARLY])
        pl.semaphore_wait(reach_sem.at[lm - 1], 1)
        send_down(HELPER)
        remote(dn_hbm.at[pl.ds(share(x), fh), :], wdn.at[dn_rows(HELPER), own], 6, one_sem.at[4], at(MAIN))
        arrived(gi.at[0:2], local_sem.at[1])
        arrived(unit[0 : up_units(HELPER) + NC], send_sem.at[2])
        arrived(unit[0 : 2 * (nx - 1) * len(FORWARDED)], send_sem.at[3])
        arrived(unit[0 : nx * NC], send_sem.at[6])
        arrived(unit[0:4], one_sem.at[6])
        arrived(st2.at[0 : nz * nx], one_sem.at[7])
        finish()

    def main():
        greeted = enter(
            [(MAIN, z, xs[dx], ys[dj]) for dj, dx in pairs] + [at(MAIN, dz) for dz in (1, nz - 1)]
            + [at(HELPER, 0, dx) for dx in range(nx)] + [(HELPER, z, x, yw)]
        )
        pltpu.make_async_copy(res_hbm, raw.at[x, q], local_sem.at[0]).start()
        for src, dst in ((gi_hbm, gi.at[x]), (si_hbm, si.at[x]), (go_hbm, go), (so_hbm, so)):
            pltpu.make_async_copy(src, dst, local_sem.at[1]).start()
        for c in range(NC // 2, NC):
            pltpu.make_async_copy(up_hbm.at[:, up_cols(c, x)], wup.at[c, own, :], local_sem.at[2]).start()
        src = dn_hbm.at[pl.ds(share(x), fh), :]
        pltpu.make_async_copy(src, wdn.at[dn_rows(MAIN), own], local_sem.at[2]).start()
        arrived(unit[0:2], local_sem.at[0])
        arrived(gi, local_sem.at[1])
        st0[0] = of_shard(raw[x, q].astype(F32))
        greeted()

        for dj, dx in pairs:
            remote(st0.at[0], st0.at[dj * nx + dx], 11, one_sem.at[3], (MAIN, z, xs[dx], ys[dj]))
        halves = [slice(part * tokens // 2, (part + 1) * tokens // 2) for part in range(2)]
        for part, place in enumerate(halves):
            for dx in (2, 1, 3):
                block = raw.at[x, q, place, :]
                remote(block, block, 0, raw_sem.at[2 * dx + part], at(MAIN, 0, dx))
        mate = (MAIN, z, x, ys[1])
        remote(raw.at[x, q], raw.at[x, q], 0, raw_sem.at[0], mate)
        for dx in range(1, nx):
            remote(gi.at[x], gi.at[x], 1, one_sem.at[0], at(MAIN, 0, dx))
            remote(si.at[x], si.at[x], 8, one_sem.at[1], at(MAIN, 0, dx))
        send_up(MAIN, range(NC))

        for k in range(lm - 1):
            for dz in (1, nz - 1):
                pl.semaphore_signal(reach_sem.at[k], inc=1, device_id=at(MAIN, dz), device_id_type=MESH)
            pl.semaphore_wait(reach_sem.at[k], 2)

        arrived(st0.at[1 : 2 * nx], one_sem.at[3])
        for dj in range(2):
            st1[z, qs[dj]] = jnp.concatenate(pool(st0[dj * nx : (dj + 1) * nx], width), axis=0)
        for dz in FAR[:-1]:
            remote(st1.at[z], st1.at[z], 9, one_sem.at[2], at(MAIN, dz))
        for part, place in enumerate(halves):
            for dx in (1, 3, 2):
                block = raw.at[xs[nx - dx], q, place, :]
                arrived(block, raw_sem.at[2 * dx + part])
                remote(block, block, 0, raw_sem.at[0], mate)
        arrived(gi.at[1:nx], one_sem.at[0])
        arrived(si.at[1:nx], one_sem.at[1])
        arrived(unit[0 : 2 * nx], raw_sem.at[0])
        arrived(st1.at[1:nz], one_sem.at[2])
        for j in range(2):
            mean, scale = combine(st1[:, j], depth)
            mean, scale = row_to_lanes(mean), row_to_lanes(scale)
            for k in range(nx):
                v = (raw[k, j].astype(F32) - mean) * scale * gi[k] + si[k]
                normed[j * nq : (j + 1) * nq, :, k * width : (k + 1) * width] = v.astype(BF16).reshape(nq, rows, width)

        def products(ks, c):
            left = jnp.concatenate([normed[zs[k]] for k in ks], axis=0)
            value = jnp.dot(left, wup[c], preferred_element_type=F32)
            return [value[i * rows : (i + 1) * rows] for i in range(len(ks))]

        def active(c, s):
            return [di for di in range(2) if s < hops(c, di, nz)]

        def target(c, di, s):
            ahead = hops(c, di, nz) - s
            return ahead if di == 0 else nz - ahead

        def pass_on(c, di, s, value):
            rsb[c, s, di] = value.astype(BF16)
            remote(rsb.at[c, s, di], rrb.at[c, s, di], 4, ring_sem.at[c, s % 2], at(MAIN, 1 if di == 0 else nz - 1))

        def spread(c, di, s):
            block = unit[c * nz + (zs[nz - s if s else 0] if di == 0 else zs[s])]
            remote(block, block, 5, ring_sem.at[c, (s + 2) % 3], at(MAIN, 1 if di == 0 else nz - 1))

        arrived(unit[0 : 2 * NC], local_sem.at[2])
        for c in ORDER:
            arrived(unit[0 : 2 * (nx - 1) + (2 if c < NC // 2 else 0)], up_sem.at[c])
            near = [target(c, di, s) for s in range(2) for di in range(2)]
            values = products(near, c)
            for di in range(2):
                pass_on(c, di, 0, values[di])
                pbuf[c, near[2 + di]] = values[2 + di]
        pl.semaphore_signal(reach_sem.at[lm - 1], inc=1, device_id=at(HELPER), device_id_type=MESH)
        send_down(MAIN)
        for s in range(1, lm + 1):
            for c in ORDER:
                arrived(rrb.at[c, 0, 0 : len(active(c, s - 1))], ring_sem.at[c, (s - 1) % 2])
                if s < lm:
                    for di in active(c, s):
                        pass_on(c, di, s, pbuf[c, target(c, di, s)] + rrb[c, s - 1, di].astype(F32))
                    if s == 1:
                        far = [target(c, di, t) for t in range(2, lm) for di in active(c, t)] + [0]
                        for k, value in zip(far, products(far, c)):
                            pbuf[c, k] = value
                else:
                    value = pbuf[c, 0]
                    for di in range(2):
                        value = value + rrb[c, hops(c, di, nz) - 1, di].astype(F32)
                    hid[c * nz + z] = jnp.square(jnp.maximum(value, 0.0)).astype(BF16)
                    for di in range(2):
                        spread(c, di, 0)

        def down(c, ks):
            place = ORDER.index(c)
            if place % 2 == 0:
                return
            pair = (ORDER[place - 1], c)
            halves = [jnp.concatenate([hid[half * nz + zs[k]] for k in ks], axis=0) for half in pair]
            right = jnp.concatenate([wdn[half * cw : (half + 1) * cw, :] for half in pair], axis=0)
            value = jnp.dot(jnp.concatenate(halves, axis=1), right, preferred_element_type=F32)
            for i, k in enumerate(ks):
                part = value[i * rows : (i + 1) * rows]
                acc[k] = part if place == 1 else acc[k] + part

        def branch(ks):
            for k in ks:
                o = zs[k]
                sb[o] = acc[k].astype(BF16)
                j, i = lax.div(o, nq), lax.rem(o, nq)
                dj = lax.rem(j + q, 2)
                for dx in (2, 1, 3, 0):
                    cols = pl.ds(pl.multiple_of(xs[dx] * width, width), width)
                    send = functools.partial(
                        remote, sb.at[o, :, cols], rb.at[dj, dx, i], 7, one_sem.at[5], (MAIN, z, xs[dx], y - q + j)
                    )
                    if dx:
                        send()
                    else:
                        pl.when(dj != 0)(send)

        stages = [(0, 1, nz - 1)] + [(k, nz - k) for k in range(2, lm)] + [(lm,)]
        for s in range(1, lm + 1):
            if s == 2:
                arrived(unit[0 : NC * (nx - 1) * 2 + NC], one_sem.at[4])
            for c in ORDER:
                arrived(unit[0 : len(active(c, s - 1))], ring_sem.at[c, (s + 1) % 3])
                for di in active(c, s):
                    spread(c, di, s)
                if s > 1:
                    down(c, stages[s - 2] if s < lm else stages[s - 1])
            if 1 < s < lm:
                branch(stages[s - 2])
            if s == lm - 1:
                for c in ORDER:
                    down(c, stages[s - 1])
                branch(stages[s - 1])
        branch(stages[lm - 1])

        blocks = pl.ds(pl.multiple_of(q * nq, nq), nq)
        total = 2.0**0.25 * normed[blocks, :, own].astype(F32) + sb[blocks, :, own].astype(F32)
        arrived(unit[0 : 2 * len(pairs)], one_sem.at[5])
        for dj, dx in pairs:
            total = total + rb[dj, dx].astype(F32)
        total = total.reshape(tokens, width)
        st2[0] = of_shard(total)
        tot[...] = total
        for core in (MAIN, HELPER):
            for dz in FAR:
                for dx in (2, 1, 3, 0):
                    k = dz * nx + dx
                    if k or core == HELPER:
                        remote(st2.at[0], st2.at[k], 10, one_sem.at[7], at(core, dz, dx))
            if core == MAIN:
                remote(tot, tot, 0, one_sem.at[6], at(HELPER))
        arrived(st2.at[1 : nz * nx], one_sem.at[7])
        finish()

        for group, ref in (
            (0, unit[0 : 2 * len(pairs) + 4]),
            (1, gi.at[1:nx]),
            (8, si.at[1:nx]),
            (2, unit[0 : up_units(MAIN)]),
            (4, unit[0 : len(pairs) * NC]),
            (5, unit[0 : len(pairs) * NC]),
            (6, unit[0 : (nx - 1) * NC]),
            (7, unit[0 : 2 * len(pairs)]),
            (9, st1.at[1:nz]),
            (10, st2.at[1 : 2 * nz * nx]),
            (11, st0.at[1 : 2 * nx]),
        ):
            arrived(ref, send_sem.at[group])

    pl.when(r == MAIN)(main)
    pl.when(r == HELPER)(helper)


def per_device(nz, nx, residual_in, gain_in, shift_in, up_weight, down_weight, gain_out, shift_out):
    tokens, width = residual_in.shape
    nq, depth = nz // 2, nx * width
    rows = tokens // nq
    fc = up_weight.shape[1] // nx
    cw = fc // NC
    dma = pltpu.SemaphoreType.DMA
    row = (1, width)
    return pl.pallas_call(
        functools.partial(kernel, nz, nx),
        out_shape=pltpu.VMEM((tokens, width), BF16),
        in_specs=[pl.BlockSpec(memory_space=pl.ANY)] * 7,
        out_specs=pl.BlockSpec(memory_space=pltpu.VMEM),
        scratch_shapes=[
            pltpu.VMEM((nx, 2, tokens, width), BF16),
            pltpu.VMEM((nx, *row), F32),
            pltpu.VMEM((nx, *row), F32),
            pltpu.VMEM(row, F32),
            pltpu.VMEM(row, F32),
            pltpu.VMEM((NC, depth, cw), BF16),
            pltpu.VMEM((fc, depth), BF16),
            pltpu.VMEM((2 * nx, 2, tokens), F32),
            pltpu.VMEM((nz, 2, 2, tokens), F32),
            pltpu.VMEM((nz, rows, depth), BF16),
            pltpu.VMEM((NC, nz, rows, cw), F32),
            pltpu.VMEM((NC, nq, 2, rows, cw), BF16),
            pltpu.VMEM((NC, nq, 2, rows, cw), BF16),
            pltpu.VMEM((NC * nz, rows, cw), BF16),
            pltpu.VMEM((nz, rows, depth), F32),
            pltpu.VMEM((nz, rows, depth), BF16),
            pltpu.VMEM((2, nx, nq, rows, width), BF16),
            pltpu.VMEM((2 * nz * nx, 2, tokens), F32),
            pltpu.VMEM((tokens, width), F32),
            dma((3,)),
            dma((12,)),
            dma((2 * nx,)),
            dma((NC + len(FORWARDED),)),
            dma((8,)),
            dma((NC, 3)),
            pltpu.SemaphoreType.REGULAR((nq,)),
        ],
        compiler_params=pltpu.CompilerParams(collective_id=0, has_side_effects=True),
    )(
        residual_in, gain_in.reshape(row), shift_in.reshape(row), up_weight, down_weight,
        gain_out.reshape(row), shift_out.reshape(row),
    )


def solution(mesh):
    nz, nx = 8, 4
    split = Mesh(
        mesh.devices.reshape(mesh.shape["ra"], nz, nx, mesh.shape["dp"]), ("ra", "cb_0", "cb_1", "dp")
    )
    placed = (P("dp", CB), P(CB), P(CB), P(CB, "ra"), P("ra", CB), P(CB), P(CB))
    return jax.shard_map(
        functools.partial(per_device, nz, nx), mesh=split, in_specs=placed, out_specs=P("dp", CB), check_vma=False
    )
```

```python
import functools

import jax
import jax.numpy as jnp
from jax import lax
from jax.experimental import pallas as pl
from jax.experimental.pallas import tpu as pltpu
from jax.sharding import Mesh
from jax.sharding import PartitionSpec as P

CB = ("cb_0", "cb_1")
MESH = pl.DeviceIdType.MESH
NC = 8
ORDER = (0, 5, 1, 6, 4, 3, 2, 7)
FORWARDED = (0, 1, 4, 2)
EARLY = (0, 1, 2)
FAR = (4, 3, 5, 2, 6, 1, 7, 0)
MAIN, HELPER = 1, 0
EPS = 1e-05
F32 = jnp.float32
BF16 = jnp.bfloat16


def hops(c, di, nz):
    return nz // 2 - (ORDER.index(c) + di) % 2


def columns_to_rows(a, b):
    n = a.shape[0]
    lane = lax.broadcasted_iota(jnp.int32, (n, 128), 1)
    both = jnp.where(lane == 0, a, jnp.where(lane == 1, b, 0.0))
    return both.T[0:2, :]


def row_to_lanes(row):
    return jnp.broadcast_to(row, (128, row.shape[1])).T


def pool(stats, count):
    sums, squares = stats[:, 0, :], stats[:, 1, :]
    total = jnp.sum(sums, axis=0, keepdims=True)
    apart = sums / count - total / (stats.shape[0] * count)
    return total, jnp.sum(squares, axis=0, keepdims=True) + count * jnp.sum(apart * apart, axis=0, keepdims=True)


def combine(stats, count):
    total, square = pool(stats, count)
    whole = stats.shape[0] * count
    return total / whole, lax.rsqrt(square / whole + EPS)


def of_shard(values):
    sums = jnp.sum(values, axis=1, keepdims=True)
    apart = values - sums / values.shape[1]
    return columns_to_rows(sums, jnp.sum(apart * apart, axis=1, keepdims=True))


def kernel(
    nz, nx, res_hbm, gi_hbm, si_hbm, up_hbm, dn_hbm, go_hbm, so_hbm, out_ref,
    raw, gi, si, go, so, wup, wdn, st0, st1, normed, pbuf, rsb, rrb, hid, acc, sb, rb, st2, tot,
    local_sem, send_sem, raw_sem, up_sem, one_sem, ring_sem, reach_sem,
):
    tokens, width = res_hbm.shape
    nq = nz // 2
    rows = tokens // nq
    depth = nx * width
    fc = wdn.shape[0]
    fh = fc // 2
    cw = fc // NC
    lm = nz // 2
    hw = width // 2

    r = lax.axis_index("ra")
    z = lax.axis_index("cb_0")
    x = lax.axis_index("cb_1")
    y = lax.axis_index("dp")
    q = lax.rem(y, 2)
    pf = lax.rem(lax.div(y + 1, 2), 2)
    w = lax.div(y, 2)
    yw = 3 - y
    xs = [lax.rem(x + k, nx) for k in range(nx)]
    zs = [lax.rem(z + k, nz) for k in range(nz)]
    ys = [y, y + 1 - 2 * q]
    qs = [q, 1 - q]
    pairs = [(dj, dx) for dx in (2, 1, 3, 0) for dj in (1, 0) if dx or dj]
    own = pl.ds(pl.multiple_of(x * width, width), width)
    unit = hid.at

    def at(core, dz=0, dx=0):
        return (core, zs[dz], xs[dx], y)

    def enter(peers):
        barrier = pltpu.get_barrier_semaphore()
        for peer in peers:
            pl.semaphore_signal(barrier, inc=1, device_id=peer, device_id_type=MESH)
        return lambda: pl.semaphore_wait(barrier, len(peers))

    def remote(src, dst, group, recv, peer):
        copy = pltpu.make_async_remote_copy(
            src_ref=src, dst_ref=dst, send_sem=send_sem.at[group], recv_sem=recv, device_id=peer, device_id_type=MESH
        )
        copy.start()

    def arrived(ref, sem):
        pltpu.make_async_copy(ref, ref, sem).wait()

    def share(xd):
        return pl.multiple_of((xd * 2 + pf) * fh, fh)

    def up_cols(c, xd):
        return pl.ds(pl.multiple_of(share(xd) + c % (NC // 2) * cw, cw), cw)

    def up_rows(xd, part):
        return pl.ds(pl.multiple_of(xd * width + part * hw, hw), hw)

    def dn_rows(core):
        return pl.ds(core * fh, fh)

    def send_up(core, chunks):
        for c in chunks:
            if c // (NC // 2) == core:
                for dx in (2, 1, 3):
                    if c in FORWARDED:
                        part = pl.ds(pl.multiple_of(w * hw, hw), hw)
                        dst = wup.at[c, up_rows(x, w), :]
                        remote(up_hbm.at[part, up_cols(c, xs[dx])], dst, 2, up_sem.at[NC + FORWARDED.index(c)], at(HELPER, 0, dx))
                    else:
                        dst = wup.at[c, own, :]
                        remote(up_hbm.at[:, up_cols(c, xs[dx])], dst, 2, up_sem.at[c], at(MAIN, 0, dx))
                if core == HELPER:
                    remote(up_hbm.at[:, up_cols(c, x)], wup.at[c, own, :], 2, up_sem.at[c], at(MAIN))

    def up_units(core):
        return sum((nx - 1) * (1 if c in FORWARDED else 2) for c in ORDER if c // (NC // 2) == core)

    def send_down(core):
        for dx in (2, 1, 3):
            src = dn_hbm.at[pl.ds(share(xs[dx]), fh), :]
            remote(src, wdn.at[dn_rows(core), own], 6, one_sem.at[4], at(MAIN, 0, dx))

    def finish():
        mean, scale = combine(st2[0 : nz * nx], width)
        out = (tot[...] - row_to_lanes(mean)) * row_to_lanes(scale) * go[...] + so[...]
        out_ref[...] = out.astype(BF16)

    def helper():
        greeted = enter([(MAIN, z, x, yw), at(MAIN)] + [at(core, 0, dx) for dx in range(1, nx) for core in (0, 1)])
        pltpu.make_async_copy(go_hbm, go, local_sem.at[1]).start()
        pltpu.make_async_copy(so_hbm, so, local_sem.at[1]).start()
        early = [(c, dx) for c in EARLY for dx in (2, 1, 3)]
        part = pl.ds(pl.multiple_of(w * hw, hw), hw)
        for i, (c, dx) in enumerate(early):
            pltpu.make_async_copy(up_hbm.at[part, up_cols(c, xs[dx])], unit[i], local_sem.at[0]).start()
        arrived(unit[0 : len(early)], local_sem.at[0])
        greeted()
        for i, (c, dx) in enumerate(early):
            remote(unit[i], wup.at[c, up_rows(x, w), :], 2, up_sem.at[NC + FORWARDED.index(c)], at(HELPER, 0, dx))
        for c in EARLY:
            remote(up_hbm.at[:, up_cols(c, x)], wup.at[c, own, :], 2, up_sem.at[c], at(MAIN))
        for c in FORWARDED:
            arrived(unit[0 : nx - 1], up_sem.at[NC + FORWARDED.index(c)])
            for dx in range(1, nx):
                block = wup.at[c, up_rows(xs[dx], w), :]
                remote(block, block, 6, up_sem.at[c], (MAIN, z, x, yw))
            for dx in range(1, nx):
                block = wup.at[c, up_rows(xs[dx], w), :]
                remote(block, block, 6, up_sem.at[c], at(MAIN))
            if c == FORWARDED[0]:
                send_up(HELPER, [c for c in ORDER if c not in EARLY])
        pl.semaphore_wait(reach_sem.at[lm - 1], 1)
        send_down(HELPER)
        remote(dn_hbm.at[pl.ds(share(x), fh), :], wdn.at[dn_rows(HELPER), own], 6, one_sem.at[4], at(MAIN))
        arrived(gi.at[0:2], local_sem.at[1])
        arrived(unit[0 : up_units(HELPER) + NC], send_sem.at[2])
        arrived(unit[0 : 2 * (nx - 1) * len(FORWARDED) + nx * NC], send_sem.at[6])
        arrived(unit[0:4], one_sem.at[6])
        arrived(st2.at[0 : nz * nx], one_sem.at[7])
        finish()

    def main():
        greeted = enter(
            [(MAIN, z, xs[dx], ys[dj]) for dj, dx in pairs] + [at(MAIN, dz) for dz in (1, nz - 1)]
            + [at(HELPER, 0, dx) for dx in range(nx)] + [(HELPER, z, x, yw)]
        )
        pltpu.make_async_copy(res_hbm, raw.at[x, q], local_sem.at[0]).start()
        for src, dst in ((gi_hbm, gi.at[x]), (si_hbm, si.at[x]), (go_hbm, go), (so_hbm, so)):
            pltpu.make_async_copy(src, dst, local_sem.at[1]).start()
        for c in range(NC // 2, NC):
            pltpu.make_async_copy(up_hbm.at[:, up_cols(c, x)], wup.at[c, own, :], local_sem.at[2]).start()
        src = dn_hbm.at[pl.ds(share(x), fh), :]
        pltpu.make_async_copy(src, wdn.at[dn_rows(MAIN), own], local_sem.at[2]).start()
        arrived(unit[0:2], local_sem.at[0])
        arrived(gi, local_sem.at[1])
        st0[0] = of_shard(raw[x, q].astype(F32))
        greeted()

        for dj, dx in pairs:
            remote(st0.at[0], st0.at[dj * nx + dx], 0, one_sem.at[3], (MAIN, z, xs[dx], ys[dj]))
        halves = [slice(part * tokens // 2, (part + 1) * tokens // 2) for part in range(2)]
        for part, place in enumerate(halves):
            for dx in (2, 1, 3):
                block = raw.at[x, q, place, :]
                remote(block, block, 6, raw_sem.at[2 * dx + part], at(MAIN, 0, dx))
        mate = (MAIN, z, x, ys[1])
        remote(raw.at[x, q], raw.at[x, q], 6, raw_sem.at[0], mate)
        for dx in range(1, nx):
            remote(gi.at[x], gi.at[x], 1, one_sem.at[0], at(MAIN, 0, dx))
            remote(si.at[x], si.at[x], 8, one_sem.at[1], at(MAIN, 0, dx))
        send_up(MAIN, range(NC))

        for k in range(lm - 1):
            for dz in (1, nz - 1):
                pl.semaphore_signal(reach_sem.at[k], inc=1, device_id=at(MAIN, dz), device_id_type=MESH)
            pl.semaphore_wait(reach_sem.at[k], 2)

        arrived(st0.at[1 : 2 * nx], one_sem.at[3])
        for dj in range(2):
            st1[z, qs[dj]] = jnp.concatenate(pool(st0[dj * nx : (dj + 1) * nx], width), axis=0)
        for dz in FAR[:-1]:
            remote(st1.at[z], st1.at[z], 7, one_sem.at[2], at(MAIN, dz))
        for part, place in enumerate(halves):
            for dx in (1, 3, 2):
                block = raw.at[xs[nx - dx], q, place, :]
                arrived(block, raw_sem.at[2 * dx + part])
                remote(block, block, 6, raw_sem.at[0], mate)
        arrived(gi.at[1:nx], one_sem.at[0])
        arrived(si.at[1:nx], one_sem.at[1])
        arrived(unit[0 : 2 * nx], raw_sem.at[0])
        arrived(st1.at[1:nz], one_sem.at[2])
        for j in range(2):
            mean, scale = combine(st1[:, j], depth)
            mean, scale = row_to_lanes(mean), row_to_lanes(scale)
            for k in range(nx):
                v = (raw[k, j].astype(F32) - mean) * scale * gi[k] + si[k]
                normed[j * nq : (j + 1) * nq, :, k * width : (k + 1) * width] = v.astype(BF16).reshape(nq, rows, width)

        def products(ks, c):
            left = jnp.concatenate([normed[zs[k]] for k in ks], axis=0)
            value = jnp.dot(left, wup[c], preferred_element_type=F32)
            return [value[i * rows : (i + 1) * rows] for i in range(len(ks))]

        def active(c, s):
            return [di for di in range(2) if s < hops(c, di, nz)]

        def target(c, di, s):
            ahead = hops(c, di, nz) - s
            return ahead if di == 0 else nz - ahead

        def pass_on(c, di, s, value):
            rsb[c, s, di] = value.astype(BF16)
            remote(rsb.at[c, s, di], rrb.at[c, s, di], 4, ring_sem.at[c, s % 2], at(MAIN, 1 if di == 0 else nz - 1))

        def spread(c, di, s):
            block = unit[c * nz + (zs[nz - s if s else 0] if di == 0 else zs[s])]
            remote(block, block, 5, ring_sem.at[c, (s + 2) % 3], at(MAIN, 1 if di == 0 else nz - 1))

        arrived(unit[0 : 2 * NC], local_sem.at[2])
        for c in ORDER:
            arrived(unit[0 : 2 * (nx - 1) + (2 if c < NC // 2 else 0)], up_sem.at[c])
            near = [target(c, di, s) for s in range(2) for di in range(2)]
            values = products(near, c)
            for di in range(2):
                pass_on(c, di, 0, values[di])
                pbuf[c, near[2 + di]] = values[2 + di]
        pl.semaphore_signal(reach_sem.at[lm - 1], inc=1, device_id=at(HELPER), device_id_type=MESH)
        send_down(MAIN)
        for s in range(1, lm + 1):
            for c in ORDER:
                arrived(rrb.at[c, 0, 0 : len(active(c, s - 1))], ring_sem.at[c, (s - 1) % 2])
                if s < lm:
                    for di in active(c, s):
                        pass_on(c, di, s, pbuf[c, target(c, di, s)] + rrb[c, s - 1, di].astype(F32))
                    if s == 1:
                        far = [target(c, di, t) for t in range(2, lm) for di in active(c, t)] + [0]
                        for k, value in zip(far, products(far, c)):
                            pbuf[c, k] = value
                else:
                    value = pbuf[c, 0]
                    for di in range(2):
                        value = value + rrb[c, hops(c, di, nz) - 1, di].astype(F32)
                    hid[c * nz + z] = jnp.square(jnp.maximum(value, 0.0)).astype(BF16)
                    for di in range(2):
                        spread(c, di, 0)

        def down(c, ks):
            place = ORDER.index(c)
            if place % 2 == 0:
                return
            pair = (ORDER[place - 1], c)
            halves = [jnp.concatenate([hid[half * nz + zs[k]] for k in ks], axis=0) for half in pair]
            right = jnp.concatenate([wdn[half * cw : (half + 1) * cw, :] for half in pair], axis=0)
            value = jnp.dot(jnp.concatenate(halves, axis=1), right, preferred_element_type=F32)
            for i, k in enumerate(ks):
                part = value[i * rows : (i + 1) * rows]
                acc[k] = part if place == 1 else acc[k] + part

        def branch(ks):
            for k in ks:
                o = zs[k]
                sb[o] = acc[k].astype(BF16)
                j, i = lax.div(o, nq), lax.rem(o, nq)
                dj = lax.rem(j + q, 2)
                for dx in (2, 1, 3, 0):
                    cols = pl.ds(pl.multiple_of(xs[dx] * width, width), width)
                    send = functools.partial(
                        remote, sb.at[o, :, cols], rb.at[dj, dx, i], 6, one_sem.at[5], (MAIN, z, xs[dx], y - q + j)
                    )
                    if dx:
                        send()
                    else:
                        pl.when(dj != 0)(send)

        stages = [(0, 1, nz - 1)] + [(k, nz - k) for k in range(2, lm)] + [(lm,)]
        for s in range(1, lm + 1):
            if s == 2:
                arrived(unit[0 : NC * (nx - 1) * 2 + NC], one_sem.at[4])
            for c in ORDER:
                arrived(unit[0 : len(active(c, s - 1))], ring_sem.at[c, (s + 1) % 3])
                for di in active(c, s):
                    spread(c, di, s)
                if s > 1:
                    down(c, stages[s - 2] if s < lm else stages[s - 1])
            if 1 < s < lm:
                branch(stages[s - 2])
            if s == lm - 1:
                for c in ORDER:
                    down(c, stages[s - 1])
                branch(stages[s - 1])
        branch(stages[lm - 1])

        blocks = pl.ds(pl.multiple_of(q * nq, nq), nq)
        total = 2.0**0.25 * normed[blocks, :, own].astype(F32) + sb[blocks, :, own].astype(F32)
        arrived(unit[0 : 2 * len(pairs)], one_sem.at[5])
        for dj, dx in pairs:
            total = total + rb[dj, dx].astype(F32)
        total = total.reshape(tokens, width)
        st2[0] = of_shard(total)
        for core in (MAIN, HELPER):
            for dz in FAR:
                for dx in (2, 1, 3, 0):
                    k = dz * nx + dx
                    if k or core == HELPER:
                        remote(st2.at[0], st2.at[k], 3, one_sem.at[7], at(core, dz, dx))
            if core == MAIN:
                tot[...] = total
                remote(tot, tot, 6, one_sem.at[6], at(HELPER))
        arrived(st2.at[1 : nz * nx], one_sem.at[7])
        finish()

        for group, ref in (
            (1, gi.at[1:nx]),
            (8, si.at[1:nx]),
            (2, unit[0 : up_units(MAIN)]),
            (4, unit[0 : len(pairs) * NC]),
            (5, unit[0 : len(pairs) * NC]),
            (6, unit[0 : (nx - 1) * NC + 4 * len(pairs) + 4]),
            (7, st1.at[1:nz]),
            (3, st2.at[1 : 2 * nz * nx]),
            (0, st0.at[1 : 2 * nx]),
        ):
            arrived(ref, send_sem.at[group])

    pl.when(r == MAIN)(main)
    pl.when(r == HELPER)(helper)


def per_device(nz, nx, residual_in, gain_in, shift_in, up_weight, down_weight, gain_out, shift_out):
    tokens, width = residual_in.shape
    nq, depth = nz // 2, nx * width
    rows = tokens // nq
    fc = up_weight.shape[1] // nx
    cw = fc // NC
    dma = pltpu.SemaphoreType.DMA
    row = (1, width)
    return pl.pallas_call(
        functools.partial(kernel, nz, nx),
        out_shape=pltpu.VMEM((tokens, width), BF16),
        in_specs=[pl.BlockSpec(memory_space=pl.ANY)] * 7,
        out_specs=pl.BlockSpec(memory_space=pltpu.VMEM),
        scratch_shapes=[
            pltpu.VMEM((nx, 2, tokens, width), BF16),
            pltpu.VMEM((nx, *row), F32),
            pltpu.VMEM((nx, *row), F32),
            pltpu.VMEM(row, F32),
            pltpu.VMEM(row, F32),
            pltpu.VMEM((NC, depth, cw), BF16),
            pltpu.VMEM((fc, depth), BF16),
            pltpu.VMEM((2 * nx, 2, tokens), F32),
            pltpu.VMEM((nz, 2, 2, tokens), F32),
            pltpu.VMEM((nz, rows, depth), BF16),
            pltpu.VMEM((NC, nz, rows, cw), F32),
            pltpu.VMEM((NC, nq, 2, rows, cw), BF16),
            pltpu.VMEM((NC, nq, 2, rows, cw), BF16),
            pltpu.VMEM((NC * nz, rows, cw), BF16),
            pltpu.VMEM((nz, rows, depth), F32),
            pltpu.VMEM((nz, rows, depth), BF16),
            pltpu.VMEM((2, nx, nq, rows, width), BF16),
            pltpu.VMEM((2 * nz * nx, 2, tokens), F32),
            pltpu.VMEM((tokens, width), F32),
            dma((3,)),
            dma((9,)),
            dma((2 * nx,)),
            dma((NC + len(FORWARDED),)),
            dma((8,)),
            dma((NC, 3)),
            pltpu.SemaphoreType.REGULAR((nq,)),
        ],
        compiler_params=pltpu.CompilerParams(collective_id=0, has_side_effects=True),
    )(
        residual_in, gain_in.reshape(row), shift_in.reshape(row), up_weight, down_weight,
        gain_out.reshape(row), shift_out.reshape(row),
    )


def solution(mesh):
    nz, nx = 8, 4
    split = Mesh(
        mesh.devices.reshape(mesh.shape["ra"], nz, nx, mesh.shape["dp"]), ("ra", "cb_0", "cb_1", "dp")
    )
    placed = (P("dp", CB), P(CB), P(CB), P(CB, "ra"), P("ra", CB), P(CB), P(CB))
    return jax.shard_map(
        functools.partial(per_device, nz, nx), mesh=split, in_specs=placed, out_specs=P("dp", CB), check_vma=False
    )
```
